32 devices in a mesh: grp: 2 (over y), fs: 4 (over z), tp: 4 (over x, core).
Axes of the slice: x: 2, y: 2, z: 4, core: 2. Of those that a mesh axis runs over, the one named last changes fastest.
Arguments:
- inputs: bfloat16 [6144, 2048], P(('grp', 'fs'), 'tp'), parts along dimension 0, may hold values from -110 to 110, as said below
- mixer_gain: float32 [2048], replicated, may hold values from 0.1 to 1.9
- query_weight: bfloat16 [2048, 1024], P('fs', 'tp'), may hold values from -0.125 to 0.125
- key_weight: bfloat16 [2048, 1024], P('fs', 'tp'), may hold values from -0.125 to 0.125
- value_weight: bfloat16 [2048, 1024], P('fs', 'tp'), may hold values from -0.125 to 0.125
- gate_weight: bfloat16 [2048, 1024], P('fs', 'tp'), may hold values from -0.125 to 0.125
- head_gain: float32 [1024], P('tp'), may hold values from 0.1 to 1.9
- out_weight: bfloat16 [1024, 2048], P('tp', 'fs'), may hold values from -0.1875 to 0.1875
- channel_gain: float32 [2048], replicated, may hold values from 0.1 to 1.9
- up_weight: bfloat16 [2048, 5632], P('fs', 'tp'), may hold values from -0.125 to 0.125
- switch_weight: bfloat16 [2048, 5632], P('fs', 'tp'), may hold values from -0.125 to 0.125
- filter_up: float32 [3, 5632], P(None, 'tp'), may hold values from -3.5 to 3.5
- filter_switch: float32 [3, 5632], P(None, 'tp'), may hold values from -3.5 to 3.5
- down_weight: bfloat16 [5632, 2048], P('tp', 'fs'), may hold values from -0.078125 to 0.078125
Outputs:
- layer_output: bfloat16 [6144, 2048], P(('grp', 'fs'), 'tp'), parts along dimension 0
The draws below stay inside these ranges and needn't reach their ends.
There are 2 independent parts, one for each index of `grp`. The reference program is written for one: setup_inputs(seed, part) draws one part's arguments, and reference() takes and returns one part's arrays. A program takes and returns all parts, laid end to end along the dimension named above; an argument that names none is the same for every part. Nothing has to cross between parts.
Inputs may be any that keep to these rules, and one draw needn't show every extreme that they name: `inputs`: activations of one part.
All inputs are finite; a program needn't handle non-finite values.
Results may differ from the reference program's by a relative error of at most 0.012.
Values may be sent and summed in bfloat16 or wider, within the bound.
A program may use at most 64 MiB of HBM per device.

```python
import jax
import jax.numpy as jnp
from jax import lax

D = 2048
HEAD = 128
FF = 5632
KERNEL = 3
TOK_DEV = 768
RET = 1024
TOKENS = 3072
N_FS = 4
N_TP = 4


def draw_inputs(key, part):
    keys_list = jax.random.split(jax.random.fold_in(key, 11), 3)
    trend_line = jnp.log(3.0) * (jnp.arange(D, dtype=jnp.float32) / D - 0.5)
    column_scale = jnp.exp(jax.random.uniform(keys_list[1], (D,), jnp.float32, -1.15, 1.15) + trend_line)
    noise_field = jnp.clip(jax.random.normal(keys_list[0], (TOKENS, D), jnp.float32), -6.0, 6.0)
    row_scale = jnp.exp(jax.random.uniform(keys_list[2], (TOKENS, 1), jnp.float32, -1.15, 1.15))
    return (noise_field * row_scale * column_scale[None, :]).astype(jnp.bfloat16)


def shard_levels(stream_key, shape, cuts, smallest, top_value):
    def one(dim, parts):
        heights = jax.random.uniform(jax.random.fold_in(jax.random.fold_in(stream_key, 6), dim), (parts,), jnp.float32, smallest / len(cuts), top_value / len(cuts))
        return jnp.repeat(jnp.exp(heights), shape[dim] // parts).reshape((-1,) + (1,) * (len(shape) - dim - 1))

    level = one(*cuts[0])
    for cut in cuts[1:]:
        level = level * one(*cut)
    return level


def scatter_about(stream_key, dims, scale, limit, cuts=(), held_as=jnp.bfloat16):
    entries = scale * jax.random.normal(stream_key, dims, jnp.float32)
    if cuts:
        entries = entries * shard_levels(stream_key, dims, cuts, -0.22, 0.18)
    return jnp.clip(entries, -limit, limit).astype(held_as)


def setup_inputs(seed: int = 0, part: int = 0) -> dict:
    keys = jax.random.split(jax.random.key(seed), 15)
    part_splits = jax.random.split(jax.random.fold_in(keys[14], part), 15)
    inputs = draw_inputs(jax.random.fold_in(jax.random.fold_in(keys[14], part), 71), part)
    mixer_gain = jnp.clip(1.0 + 0.18 * jax.random.normal(keys[1], (D,), jnp.float32), 0.1, 1.9)
    query_weight = scatter_about(keys[2], (D, RET), D ** -0.5, 0.125, ((0, 4), (1, 4)))
    key_weight = scatter_about(keys[3], (D, RET), D ** -0.5, 0.125, ((0, 4), (1, 4)))
    value_weight = scatter_about(keys[4], (D, RET), D ** -0.5, 0.125, ((0, 4), (1, 4)))
    gate_weight = scatter_about(keys[5], (D, RET), D ** -0.5, 0.125, ((0, 4), (1, 4)))
    head_gain = jnp.clip(1.0 + 0.18 * jax.random.normal(keys[6], (RET,), jnp.float32), 0.1, 1.9)
    out_weight = scatter_about(keys[7], (RET, D), RET ** -0.5, 0.1875, ((0, 4), (1, 4)))
    channel_gain = jnp.clip(1.0 + 0.18 * jax.random.normal(keys[8], (D,), jnp.float32), 0.1, 1.9)
    up_weight = scatter_about(keys[9], (D, FF), D ** -0.5, 0.125, ((0, 4), (1, 4)))
    switch_weight = scatter_about(keys[10], (D, FF), D ** -0.5, 0.125, ((0, 4), (1, 4)))
    filter_up = scatter_about(keys[11], (KERNEL, FF), KERNEL ** -0.5, 3.5, ((1, 4),), jnp.float32)
    filter_switch = scatter_about(keys[12], (KERNEL, FF), KERNEL ** -0.5, 3.5, ((1, 4),), jnp.float32)
    down_weight = scatter_about(keys[13], (FF, D), FF ** -0.5, 0.078125, ((0, 4), (1, 4)))
    return dict(inputs=inputs, mixer_gain=mixer_gain, query_weight=query_weight, key_weight=key_weight, value_weight=value_weight, gate_weight=gate_weight, head_gain=head_gain, out_weight=out_weight, channel_gain=channel_gain, up_weight=up_weight, switch_weight=switch_weight, filter_up=filter_up, filter_switch=filter_switch, down_weight=down_weight)


epsilon = 1e-06

def row_norm(row_block, gain_vector):
    values = row_block.astype(jnp.float32)
    scaled = values * lax.rsqrt(lax.optimization_barrier(jnp.mean(values * values, axis=-1, keepdims=True)) + epsilon)
    return (scaled * gain_vector.astype(jnp.float32)).astype(jnp.bfloat16)

def rotate(field, positions):
    half_width = field.shape[-1] // 2
    frequency = 10000.0 ** (-jnp.arange(half_width, dtype=jnp.float32) * 2.0 / field.shape[-1])
    angles = positions.astype(jnp.float32)[:, None] * frequency[None, :]
    cosine = jnp.cos(angles)[:, None, :]
    sine_part = jnp.sin(angles)[:, None, :]
    first_half = field[..., :half_width]
    second_half = field[..., half_width:]
    return jnp.concatenate([first_half * cosine - second_half * sine_part, first_half * sine_part + second_half * cosine], axis=-1)

def decays(first_head, count, positions):
    head_ids = (first_head + jnp.arange(count, dtype=jnp.int32)).astype(jnp.float32)
    log_decay = jnp.log1p(-jnp.exp2(-5.0 - head_ids))
    causal = positions[:, None] >= positions[None, :]
    distance = jnp.where(causal, positions[:, None] - positions[None, :], 0).astype(jnp.float32)
    return jnp.where(causal[None], jnp.exp(log_decay[:, None, None] * distance[None]), 0.0)

def retention(query_rows, key_rows, value_rows, gate_rows, gain_vector):
    length = query_rows.shape[0]
    count = query_rows.shape[1] // HEAD
    positions = jnp.arange(length, dtype=jnp.int32)
    query_rot = rotate(query_rows.astype(jnp.float32).reshape(length, count, HEAD), positions).astype(jnp.bfloat16)
    key_rot = rotate(key_rows.astype(jnp.float32).reshape(length, count, HEAD), positions).astype(jnp.bfloat16)
    decay_table = decays(0, count, positions)
    scores = jnp.einsum('thd,shd->hts', query_rot.astype(jnp.float32), key_rot.astype(jnp.float32))
    weights = (scores * HEAD ** (-0.5) * decay_table).astype(jnp.bfloat16)
    values = value_rows.reshape(length, count, HEAD).astype(jnp.float32)
    retained = jnp.einsum('hts,shd->thd', weights.astype(jnp.float32), values)
    normalized = retained * lax.rsqrt(lax.optimization_barrier(jnp.mean(retained * retained, axis=-1, keepdims=True)) + epsilon)
    gated_rows = normalized.reshape(length, count * HEAD) * gain_vector * jax.nn.silu(gate_rows.astype(jnp.float32))
    return gated_rows.astype(jnp.bfloat16)

def causal_conv(row_block, tap_weights, length):
    sequences = row_block.astype(jnp.float32).reshape(-1, length, row_block.shape[1])
    width_taps = tap_weights.shape[0]
    padded = jnp.pad(sequences, ((0, 0), (width_taps - 1, 0), (0, 0)))
    result = jnp.zeros_like(sequences)
    for tap_index in range(width_taps):
        result = result + padded[:, tap_index:tap_index + length] * tap_weights[tap_index].astype(jnp.float32)
    return result.reshape(row_block.shape)

def grouped_sum(left_side, right_side, groups):
    block_width = left_side.shape[1] // groups
    result = jnp.zeros((left_side.shape[0], right_side.shape[1]), jnp.float32)
    for group_index in range(groups):
        lower = group_index * block_width
        part_sum = jnp.dot(left_side[:, lower:lower + block_width], right_side[lower:lower + block_width], preferred_element_type=jnp.float32)
        result = result + lax.optimization_barrier(part_sum.astype(jnp.bfloat16)).astype(jnp.float32)
    return result

def reference(inputs, mixer_gain, query_weight, key_weight, value_weight, gate_weight, head_gain, out_weight, channel_gain, up_weight, switch_weight, filter_up, filter_switch, down_weight):
    normed = row_norm(inputs, mixer_gain)
    projected = [jnp.dot(normed, matrix, preferred_element_type=jnp.float32).astype(jnp.bfloat16) for matrix in (query_weight, key_weight, value_weight, gate_weight)]
    shaped = tuple((block.reshape(N_FS, TOK_DEV, block.shape[1]) for block in projected))

    def one_sequence(pieces):
        return retention(pieces[0], pieces[1], pieces[2], pieces[3], head_gain)
    head_out = lax.map(one_sequence, shaped).reshape(inputs.shape[0], -1)
    mixer_sum = grouped_sum(head_out, out_weight, N_TP)
    mixed_rows = (inputs.astype(jnp.float32) + mixer_sum).astype(jnp.bfloat16)
    channel_normed = row_norm(mixed_rows, channel_gain)
    lifted = jnp.dot(channel_normed, up_weight, preferred_element_type=jnp.float32).astype(jnp.bfloat16)
    switched = jnp.dot(channel_normed, switch_weight, preferred_element_type=jnp.float32).astype(jnp.bfloat16)
    lift_mixed = causal_conv(lifted, filter_up, TOK_DEV)
    switch_mixed = causal_conv(switched, filter_switch, TOK_DEV)
    hidden = (lift_mixed * jax.nn.silu(switch_mixed)).astype(jnp.bfloat16)
    channel_sum = grouped_sum(hidden, down_weight, N_TP)
    return (mixed_rows.astype(jnp.float32) + channel_sum).astype(jnp.bfloat16)
```

```python
import functools

import jax
import jax.numpy as jnp
from jax import lax
from jax.experimental import pallas as pl
from jax.experimental.pallas import tpu as pltpu
from jax.sharding import PartitionSpec as P

HEAD = 128
EPS = 1e-06
MESH = pl.DeviceIdType.MESH
BF = jnp.bfloat16
F32 = jnp.float32
LEAD = 3


def hidden_chunks(hidden):
    if hidden % 128:
        return [(0, hidden)]
    edges = list(range(0, hidden, 512)) + [hidden]
    return list(zip(edges[:-1], edges[1:]))


def kernel(cfg, x_hbm, mg, q_hbm, k_hbm, v_hbm, g_hbm, hg, ow_hbm, cg, up_hbm, sw_hbm, fu, fsw, dn_hbm,
           cos_ref, sin_ref, ld_ref, o_ref, *scratch):
    (wq, ob, ub, sb, db, xw, xn, xn1, qr, kr, vr, gr, ho, part, ra, st, rb, mw, mw1, lift, swit, hid,
     part1, ra1, st1, rb1, fin, loc, zs, zr, ys, yr, tks, tkr, fns, fnr) = scratch[:36]
    agx, agm, agn, rsm, rs0, rs1 = [scratch[36 + 4 * i:40 + 4 * i] for i in range(6)]
    n_g, n_f, n_t = cfg
    n_x = n_t // 2
    grp, z, t = lax.axis_index("grp"), lax.axis_index("fs"), lax.axis_index("tp")
    x, c = t // 2, t % 2
    partner = x * 2 + (1 - c)
    T, bw = x_hbm.shape
    D = bw * n_t
    RC = 256
    R = T // RC
    width = q_hbm.shape[1]
    heads = width // HEAD
    F = up_hbm.shape[1]
    fr = q_hbm.shape[0]
    slotw = ow_hbm.shape[1]
    per_block = bw // slotw
    n_j = slotw // 128
    w_j = per_block * 128
    chunks = hidden_chunks(F)

    is_end = jnp.logical_or(z == 0, z == n_f - 1)
    inner = jnp.logical_not(is_end)
    host = jnp.where(z == 0, 1, n_f - 2)
    guest = jnp.where(z == 1, 0, n_f - 1)
    second = None if n_f == 4 else jnp.logical_or(z == 1, z == n_f - 2)

    def when(cond):
        if cond is None:
            return lambda f: f()
        return pl.when(cond)

    def rows_of(r, size=RC):
        return pl.ds(r * size if isinstance(r, int) else pl.multiple_of(r * size, size), size)

    barrier = pltpu.get_barrier_semaphore()
    friends = [(grp, lax.rem(z + 1, n_f), t), (grp, lax.rem(z + n_f - 1, n_f), t), (grp, z, partner)]
    friends += [(lax.rem(grp + d, n_g), z, t) for d in range(1, n_g)]
    friends += [(grp, z, lax.rem(x + d, n_x) * 2 + c) for d in range(1, n_x)]
    for f in friends:
        pl.semaphore_signal(barrier, inc=1, device_id=f, device_id_type=MESH)

    zrow = pl.multiple_of(z * fr, fr)
    zcol = pl.multiple_of(z * 128, 128)
    local = [pltpu.make_async_copy(x_hbm, xw.at[t], loc.at[0])]
    for i, w in enumerate((q_hbm, k_hbm, v_hbm, g_hbm)):
        local.append(pltpu.make_async_copy(
            w, wq.at[pl.ds(zrow, fr), pl.ds(i * width, width)], loc.at[1 + i]))
    local.append(pltpu.make_async_copy(ow_hbm, ob.at[z], loc.at[5]))
    local.append(pltpu.make_async_copy(up_hbm, ub.at[pl.ds(zrow, fr), :], loc.at[6]))
    local.append(pltpu.make_async_copy(sw_hbm, sb.at[pl.ds(zrow, fr), :], loc.at[7]))
    for j in range(n_j):
        local.append(pltpu.make_async_copy(
            dn_hbm.at[:, pl.ds(j * 128, 128)], db.at[j, :, pl.ds(zcol, 128)], loc.at[8 + j]))
    for cp in local:
        cp.start()

    open_copies = [[]]

    def go(cp, cond=None):
        when(cond)(cp.start)
        open_copies[-1].append((cond, cp))

    def recv(cp, cond=None):
        when(cond)(cp.wait_recv)

    def drain():
        for cond, cp in open_copies[-1]:
            when(cond)(cp.wait_send)
        open_copies[-1].clear()

    pieces = []

    def add_rows(name, buf, slotted, shard, cols=None):
        half = shard // n_g
        count = 2 if name == "qkvg" and half % 32 == 0 else 1
        size = half // count
        for j in range(count):
            def ref(src, owner, j=j):
                if slotted:
                    return buf.at[src, pl.ds(pl.multiple_of(owner * half + j * size, size), size), :]
                rows = pl.ds(pl.multiple_of(src * shard + owner * half + j * size, size), size)
                return buf.at[rows, :] if cols is None else buf.at[rows, pl.ds(cols[0], cols[1] - cols[0])]
            pieces.append((name, ref))

    add_rows("qkvg", wq, False, fr)
    add_rows("out", ob, True, ow_hbm.shape[0])
    for k, cols in enumerate(chunks):
        for buf in (ub, sb):
            add_rows("ff%d" % k, buf, False, fr, cols if len(chunks) > 1 else None)
    for j in range(n_j):
        def down_ref(src, owner, j=j):
            half = F // n_g
            return db.at[j, pl.ds(pl.multiple_of(owner * half, half), half),
                         pl.ds(pl.multiple_of(src * 128, 128), 128)]
        pieces.append(("down%d" % j, down_ref))
    n_p = len(pieces)
    first_ff = min(i for i, pc in enumerate(pieces) if pc[0] == "ff0")

    def z_copy(p, src, step, way):
        ref = pieces[p][1](src, grp)
        return pltpu.make_async_remote_copy(
            src_ref=ref, dst_ref=ref, send_sem=zs.at[p, 2 * step + way], recv_sem=zr.at[p, src],
            device_id=(grp, z + (1 if way == 0 else -1), t), device_id_type=MESH)

    def y_copy(p, src, d):
        ref = pieces[p][1](src, grp)
        return pltpu.make_async_remote_copy(
            src_ref=ref, dst_ref=ref, send_sem=ys.at[p, src * n_g + d], recv_sem=yr.at[p, src * n_g + grp],
            device_id=(lax.rem(grp + d, n_g), z, t), device_id_type=MESH)

    def other_half(p, d):
        owner = lax.rem(grp + d, n_g)
        ref = pieces[p][1](z, owner)
        return pltpu.make_async_remote_copy(
            src_ref=ref, dst_ref=ref, send_sem=ys.at[p, z * n_g + d], recv_sem=yr.at[p, z * n_g + owner],
            device_id=(grp, host, t), device_id_type=MESH)

    def onward(p, way):
        edge = 1 if p >= first_ff else 0
        return z < n_f - 1 - edge if way == 0 else z > edge

    def own(p):
        for way in (0, 1):
            go(z_copy(p, z, 0, way), onward(p, way))
        if p >= first_ff:
            for d in range(1, n_g):
                go(other_half(p, d), is_end)

    def event(p, s):
        feed = p >= first_ff
        for way in (0, 1):
            src = z - s if way == 0 else z + s
            here = (src >= 0) if way == 0 else (src < n_f)
            if feed:
                here = jnp.logical_and(here, inner)
            safe = jnp.clip(src, 0, n_f - 1)
            recv(z_copy(p, safe, s, way), here)
            go(z_copy(p, safe, s, way), jnp.logical_and(here, onward(p, way)))
            share = here
            if feed and s == 1:
                share = jnp.logical_and(here, z != (1 if way == 0 else n_f - 2))
            for d in range(1, n_g):
                go(y_copy(p, safe, d), share)

    def arrive(p):
        for s in range(1, n_f):
            src = lax.rem(z + s, n_f)
            for d in range(1, n_g):
                owner = lax.rem(grp + d, n_g)
                ref = pieces[p][1](src, owner)
                pltpu.make_async_remote_copy(
                    src_ref=ref, dst_ref=ref, send_sem=ys.at[p, src * n_g],
                    recv_sem=yr.at[p, src * n_g + owner],
                    device_id=(owner, z, t), device_id_type=MESH).wait_recv()

    state = {"own": 0, "ev": 0}
    order = [(p, s) for p in range(n_p) for s in range(1, n_f - 1 if p >= first_ff else n_f)]

    def send_own(upto):
        while state["own"] < min(upto, n_p):
            own(state["own"])
            state["own"] += 1

    def pump(count=1):
        for _ in range(count):
            if state["ev"] < len(order):
                p, s = order[state["ev"]]
                send_own(p + LEAD)
                event(p, s)
                state["ev"] += 1

    def arrive_all(name):
        last = max(i for i, pc in enumerate(pieces) if pc[0] == name)
        while state["ev"] < len(order) and order[state["ev"]][0] <= last:
            pump()
        for i, pc in enumerate(pieces):
            if pc[0] == name:
                arrive(i)

    def ag_copy(buf, src_x, r, dest, ssem, rsem):
        ref = buf.at[src_x * 2 + c, rows_of(r), :]
        return pltpu.make_async_remote_copy(
            src_ref=ref, dst_ref=ref, send_sem=ssem, recv_sem=rsem,
            device_id=(grp, z, dest), device_id_type=MESH)

    def ag_start(buf, r, sems, cond=None):
        s1, r1, s2, r2 = sems
        for d in range(1, n_x):
            go(ag_copy(buf, x, r, lax.rem(x + d, n_x) * 2 + c, s1.at[d, r], r1.at[x, r]), cond)
        go(ag_copy(buf, x, r, partner, s2.at[x, r], r2.at[x, r]), cond)

    def ag_forward(buf, r, sems, cond=None):
        s1, r1, s2, r2 = sems
        for d in range(1, n_x):
            sx = lax.rem(x + d, n_x)
            recv(ag_copy(buf, sx, r, partner, s1.at[d, r], r1.at[sx, r]), cond)
            go(ag_copy(buf, sx, r, partner, s2.at[sx, r], r2.at[sx, r]), cond)

    def ag_finish(buf, r, sems, cond=None):
        s1, r1, s2, r2 = sems
        for sx in range(n_x):
            ref = buf.at[sx * 2 + (1 - c), rows_of(r), :]
            recv(pltpu.make_async_remote_copy(
                src_ref=ref, dst_ref=ref, send_sem=s2.at[sx, r], recv_sem=r2.at[sx, r],
                device_id=(grp, z, partner), device_id_type=MESH), cond)

    def norm_rows(src, gain, r, dst):
        def body(i, _):
            rows = rows_of(r * (RC // 64) + i, 64)
            total = jnp.zeros((64, 1), F32)
            for b in range(n_t):
                val = src[b, rows, :].astype(F32)
                total = total + jnp.sum(val * val, axis=-1, keepdims=True)
            inv = lax.rsqrt(total / D + EPS)
            for b in range(n_t):
                val = src[b, rows, :].astype(F32)
                dst[rows, b * bw:(b + 1) * bw] = (val * inv * gain[:, b * bw:(b + 1) * bw]).astype(BF)
            return 0
        lax.fori_loop(0, RC // 64, body, 0)

    def product(lhs, rhs, dst, block, r):
        for j in range(per_block):
            dst[block, rows_of(r), j * slotw:(j + 1) * slotw] = jnp.dot(
                lhs[rows_of(r), :], rhs[block * per_block + j], preferred_element_type=F32).astype(BF)

    def rs_copy(src_ref, dst_ref, dest, ssem, rsem):
        return pltpu.make_async_remote_copy(
            src_ref=src_ref, dst_ref=dst_ref, send_sem=ssem, recv_sem=rsem,
            device_id=(grp, z, dest), device_id_type=MESH)

    def mixer_reduce(emit):
        s1, r1, s2, r2 = rsm

        def to_partner(d, r):
            bx = lax.rem(x + d, n_x)
            return rs_copy(part.at[bx * 2 + 1 - c, rows_of(r), :], ra.at[d, rows_of(r), :],
                           partner, s1.at[d, r], r1.at[d, r])

        def across(d, r):
            return rs_copy(st.at[d - 1, rows_of(r), :], rb.at[d - 1, rows_of(r), :],
                           lax.rem(x + d, n_x) * 2 + c, s2.at[d, r], r2.at[d, r])

        sends = []

        def begin(cp):
            cp.start()
            sends.append(cp)

        def combine(d, r):
            bx = lax.rem(x + d, n_x)
            to_partner(d, r).wait_recv()
            st[d - 1, rows_of(r), :] = (part[bx * 2 + c, rows_of(r), :].astype(F32)
                                        + ra[d, rows_of(r), :].astype(F32)).astype(BF)
            begin(across(d, r))

        work = [(d, r) for d in range(1, n_x) for r in range(R)]
        prev = None
        for d, r in work + [(0, r) for r in range(R)]:
            bx = lax.rem(x + d, n_x)
            product(ho, ob, part, bx * 2 + 1 - c, r)
            begin(to_partner(d, r))
            product(ho, ob, part, bx * 2 + c, r)
            if prev is not None and prev[0] > 0:
                combine(*prev)
            prev = (d, r)
            if r % 2 == 1:
                pump(1)
        for r in range(R):
            pump(1)
            to_partner(0, r).wait_recv()
            total = part[t, rows_of(r), :].astype(F32) + ra[0, rows_of(r), :].astype(F32)
            for d in range(1, n_x):
                across(d, r).wait_recv()
                total = total + rb[d - 1, rows_of(r), :].astype(F32)
            emit(r, (xw[t, rows_of(r), :].astype(F32) + total).astype(BF))
        for cp in sends:
            cp.wait_send()

    pl.semaphore_wait(barrier, len(friends))
    local[0].wait()
    for r in range(R):
        ag_start(xw, r, agx)
    for cp in local[1:]:
        cp.wait()
    send_own(2)
    pump(1)
    for r in range(R):
        ag_forward(xw, r, agx)
    pump(1)
    for r in range(R):
        ag_finish(xw, r, agx)
        norm_rows(xw, mg, r, xn)
        pump(1)
    arrive_all("qkvg")
    send_own(5)

    def project(r):
        rows = rows_of(r)
        lhs = xn[rows, :]
        for i, dst in enumerate((qr, kr, vr, gr)):
            val = jnp.dot(lhs, wq[:, i * width:(i + 1) * width], preferred_element_type=F32).astype(BF)
            if i >= 2:
                dst[rows, :] = val
                continue
            for h in range(heads):
                part_h = val[:, h * HEAD:(h + 1) * HEAD].astype(F32)
                dst[rows, h * HEAD:(h + 1) * HEAD] = (
                    part_h * cos_ref[rows, :] + pltpu.roll(part_h, HEAD // 2, 1) * sin_ref[rows, :]).astype(BF)

    for r in range(R):
        project(r)
        pump(1)
    for h in range(heads):
        cols = slice(h * HEAD, (h + 1) * HEAD)
        for r in range(R):
            span = (r + 1) * RC
            qh = qr[r * RC:(r + 1) * RC, cols]
            scores = lax.dot_general(qh, kr[0:span, cols], (((1,), (1,)), ((), ())),
                                     preferred_element_type=F32)
            gap = (r * RC + lax.broadcasted_iota(jnp.int32, (RC, span), 0)
                   - lax.broadcasted_iota(jnp.int32, (RC, span), 1))
            causal = gap >= 0
            rate = ld_ref[h:h + 1, 0:1]
            fade = jnp.where(causal, jnp.exp(rate * jnp.where(causal, gap, 0).astype(F32)), 0.0)
            weights = (scores * HEAD ** (-0.5) * fade).astype(BF)
            kept = jnp.dot(weights, vr[0:span, cols], preferred_element_type=F32)
            kept = kept * lax.rsqrt(jnp.mean(kept * kept, axis=-1, keepdims=True) + EPS)
            gate = gr[r * RC:(r + 1) * RC, cols].astype(F32)
            ho[r * RC:(r + 1) * RC, cols] = (kept * hg[:, cols] * (gate / (1.0 + jnp.exp(-gate)))).astype(BF)
            if r != 1:
                pump(1)
    arrive_all("out")

    def token_copy(r, dest):
        return pltpu.make_async_remote_copy(
            src_ref=mw.at[t, rows_of(r), :], dst_ref=mw1.at[t, rows_of(r), :],
            send_sem=tks.at[r], recv_sem=tkr.at[r], device_id=(grp, dest, t), device_id_type=MESH)

    def emit_mixed(r, val):
        mw[t, rows_of(r), :] = val
        go(token_copy(r, host), is_end)
        ag_start(mw, r, agm, inner)

    mixer_reduce(emit_mixed)

    def fin_copy(j, dest):
        return pltpu.make_async_remote_copy(
            src_ref=fin.at[j], dst_ref=fin.at[j], send_sem=fns.at[j], recv_sem=fnr.at[j],
            device_id=(grp, dest, t), device_id_type=MESH)

    def cols_of(j):
        return slice(j * w_j, (j + 1) * w_j)

    def end_part():
        open_copies.append([])
        send_own(n_p)
        for j in range(n_j):
            fin_copy(j, host).wait_recv()
            o_ref[:, cols_of(j)] = fin[j]
        drain()
        open_copies.pop()

    def widen(weights, lhs, dst, k):
        lo, hi = chunks[k]

        def body(r, _):
            dst[pl.ds(pl.multiple_of(16 + r * RC, 16), RC), 0:hi - lo] = jnp.dot(
                lhs[rows_of(r), :], weights[:, lo:hi], preferred_element_type=F32).astype(BF)
            return 0
        lax.fori_loop(0, R, body, 0)

    def conv(q, k):
        first, last = chunks[k]
        edges = list(range(0, last - first, 256)) + [last - first]

        def body(i, _):
            for lo, hi in zip(edges[:-1], edges[1:]):
                mixed = []
                for src, taps in ((lift, fu), (swit, fsw)):
                    val = src[pl.ds(pl.multiple_of(i * 64, 64), 80), lo:hi].astype(F32)
                    acc = pltpu.roll(val, 2, 0)[16:] * taps[0:1, first + lo:first + hi]
                    acc = acc + pltpu.roll(val, 1, 0)[16:] * taps[1:2, first + lo:first + hi]
                    mixed.append(acc + val[16:] * taps[2:3, first + lo:first + hi])
                a, b = mixed
                hid[q, rows_of(i, 64), first + lo:first + hi] = (a * (b / (1.0 + jnp.exp(-b)))).astype(BF)
            return 0
        lax.fori_loop(0, T // 64, body, 0)

    sides = ((part, ra, st, rb, rs0, None), (part1, ra1, st1, rb1, rs1, second))

    def to_partner(q, d, j):
        prt, r_a, _, _, sems, _ = sides[q]
        bx = lax.rem(x + d, n_x)
        return rs_copy(prt.at[bx * 2 + 1 - c, :, pl.ds(j * w_j, w_j)], r_a.at[d, :, pl.ds(j * w_j, w_j)],
                       partner, sems[0].at[d, j], sems[1].at[d, j])

    def across(q, d, j):
        _, _, stage, r_b, sems, _ = sides[q]
        return rs_copy(stage.at[d - 1, :, pl.ds(j * w_j, w_j)], r_b.at[d - 1, :, pl.ds(j * w_j, w_j)],
                       lax.rem(x + d, n_x) * 2 + c, sems[2].at[d, j], sems[3].at[d, j])

    def down(q, j):
        prt, cond = sides[q][0], sides[q][5]

        @when(cond)
        def _():
            def body(r, _):
                val = jnp.dot(hid[q, rows_of(r), :], db[j], preferred_element_type=F32).astype(BF)
                for src in range(n_f):
                    lo = (src % per_block) * slotw + j * 128
                    prt[src // per_block, rows_of(r), lo:lo + 128] = val[:, src * 128:(src + 1) * 128]
                return 0
            lax.fori_loop(0, R, body, 0)
        for d in list(range(1, n_x)) + [0]:
            go(to_partner(q, d, j), cond)

    def combine(q, j):
        prt, r_a, stage, _, _, cond = sides[q]
        for d in range(1, n_x):
            bx = lax.rem(x + d, n_x)
            recv(to_partner(q, d, j), cond)

            @when(cond)
            def _():
                stage[d - 1, :, cols_of(j)] = (prt[bx * 2 + c, :, cols_of(j)].astype(F32)
                                               + r_a[d, :, cols_of(j)].astype(F32)).astype(BF)
            go(across(q, d, j), cond)

    def finish(q, j):
        prt, r_a, _, r_b, _, cond = sides[q]
        base = (mw, mw1)[q]
        recv(to_partner(q, 0, j), cond)
        for d in range(1, n_x):
            recv(across(q, d, j), cond)

        @when(cond)
        def _():
            total = prt[t, :, cols_of(j)].astype(F32) + r_a[0, :, cols_of(j)].astype(F32)
            for d in range(1, n_x):
                total = total + r_b[d - 1, :, cols_of(j)].astype(F32)
            val = (base[t, :, cols_of(j)].astype(F32) + total).astype(BF)
            if q == 0:
                o_ref[:, cols_of(j)] = val
            else:
                fin[j] = val
        if q == 1:
            go(fin_copy(j, guest), cond)

    def inner_part():
        open_copies.append([])
        for r in range(R):
            ag_forward(mw, r, agm)
        pump(1)
        for r in range(R):
            ag_finish(mw, r, agm)
            norm_rows(mw, cg, r, xn)
            pump(1)
        lift[0:16, :] = jnp.zeros((16, lift.shape[1]), BF)
        swit[0:16, :] = jnp.zeros((16, swit.shape[1]), BF)
        n_c = len(chunks)
        for k in range(n_c):
            if k == n_c - 1:
                for r in range(R):
                    recv(token_copy(r, guest), second)
                    ag_start(mw1, r, agn, second)
            arrive_all("ff%d" % k)
            widen(ub, xn, lift, k)
            pump(1)
            widen(sb, xn, swit, k)
            pump(1)
            conv(0, k)
            pump(1)
        for r in range(R):
            ag_forward(mw1, r, agn, second)
        for r in range(R):
            ag_finish(mw1, r, agn, second)
            when(second)(lambda: norm_rows(mw1, cg, r, xn1))
            pump(1)
        for k in range(n_c):
            when(second)(lambda: widen(ub, xn1, lift, k))
            pump(1)
            when(second)(lambda: widen(sb, xn1, swit, k))
            pump(1)
            when(second)(lambda: conv(1, k))
            pump(1)
        for j in range(n_j):
            arrive_all("down%d" % j)
            down(1, j)
            down(0, j)
            combine(1, j)
            combine(0, j)
            pump(1)
            if j > 0:
                finish(1, j - 1)
                finish(0, j - 1)
            pump(1)
        finish(1, n_j - 1)
        finish(0, n_j - 1)
        drain()
        open_copies.pop()

    kept = dict(state)
    pl.when(is_end)(end_part)
    state.update(kept)
    pl.when(inner)(inner_part)
    drain()


def on_device(cfg, inputs, mixer_gain, query_weight, key_weight, value_weight, gate_weight, head_gain,
              out_weight, channel_gain, up_weight, switch_weight, filter_up, filter_switch, down_weight):
    n_g, n_f, n_t = cfg
    n_x = n_t // 2
    T, bw = inputs.shape
    D = bw * n_t
    fr, width = query_weight.shape
    heads = width // HEAD
    F = up_weight.shape[1]
    slotw = out_weight.shape[1]
    half = HEAD // 2
    per_block = bw // slotw
    n_j = slotw // 128
    assert n_f >= 4 and slotw % 128 == 0 and bw % slotw == 0 and (n_j == 1 or per_block == 1)
    frequency = 10000.0 ** (-jnp.arange(half, dtype=F32) * 2.0 / HEAD)
    angles = jnp.arange(T, dtype=jnp.int32).astype(F32)[:, None] * frequency[None, :]
    cosine, sine = jnp.cos(angles), jnp.sin(angles)
    cos2 = jnp.concatenate([cosine, cosine], axis=1)
    sin2 = jnp.concatenate([-sine, sine], axis=1)
    ids = (lax.axis_index("tp") * heads + jnp.arange(heads, dtype=jnp.int32)).astype(F32)
    rate = jnp.broadcast_to(jnp.log1p(-jnp.exp2(-5.0 - ids))[:, None], (heads, 128))

    chunks = hidden_chunks(F)
    span = max(hi - lo for lo, hi in chunks)
    n_p = 3 + 2 * len(chunks) + n_j
    R = T // 256
    dma = pltpu.SemaphoreType.DMA
    anyspec = pl.BlockSpec(memory_space=pl.ANY)
    vspec = pl.BlockSpec(memory_space=pltpu.VMEM)
    act = pltpu.VMEM((n_t, T, bw), BF)
    flat = pltpu.VMEM((T, D), BF)
    xblk = pltpu.VMEM((n_x, T, bw), BF)
    yblk = pltpu.VMEM((n_x - 1, T, bw), BF)
    scratch = [
        pltpu.VMEM((D, 4 * width), BF),
        pltpu.VMEM((n_f,) + out_weight.shape, BF),
        pltpu.VMEM((D, F), BF),
        pltpu.VMEM((D, F), BF),
        pltpu.VMEM((n_j, F, n_f * 128), BF),
        act, flat, flat,
        pltpu.VMEM((T, width), BF), pltpu.VMEM((T, width), BF),
        pltpu.VMEM((T, width), BF), pltpu.VMEM((T, width), BF),
        pltpu.VMEM((T, width), BF),
        act, xblk, yblk, yblk,
        act, act,
        pltpu.VMEM((T + 16, span), BF), pltpu.VMEM((T + 16, span), BF), pltpu.VMEM((2, T, F), BF),
        act, xblk, yblk, yblk,
        pltpu.VMEM((n_j, T, per_block * 128), BF),
        dma((8 + n_j,)),
        dma((n_p, 2 * n_f)), dma((n_p, n_f)), dma((n_p, n_f * n_g)), dma((n_p, n_f * n_g)),
        dma((R,)), dma((R,)), dma((n_j,)), dma((n_j,)),
    ] + [dma((n_x, R))] * 16 + [dma((n_x, n_j))] * 8
    flops = 2 * T * (D * 4 * width + width * D + 3 * D * F)
    call = pl.pallas_call(
        functools.partial(kernel, cfg),
        out_shape=jax.ShapeDtypeStruct((T, bw), BF),
        in_specs=[anyspec, vspec, anyspec, anyspec, anyspec, anyspec, vspec, anyspec, vspec, anyspec, anyspec,
                  vspec, vspec, anyspec, vspec, vspec, vspec],
        out_specs=vspec,
        scratch_shapes=scratch,
        compiler_params=pltpu.CompilerParams(
            collective_id=0, has_side_effects=True, vmem_limit_bytes=67043328),
        cost_estimate=pl.CostEstimate(flops=flops, bytes_accessed=2 * (D * F * 3), transcendentals=0),
    )
    return call(inputs, mixer_gain[None, :], query_weight, key_weight, value_weight, gate_weight,
                head_gain[None, :], out_weight, channel_gain[None, :], up_weight, switch_weight,
                filter_up, filter_switch, down_weight, cos2, sin2, rate)


def solution(mesh):
    cfg = (mesh.shape["grp"], mesh.shape["fs"], mesh.shape["tp"])
    return jax.shard_map(
        functools.partial(on_device, cfg),
        mesh=mesh,
        in_specs=(
            P(("grp", "fs"), "tp"),
            P(),
            P("fs", "tp"),
            P("fs", "tp"),
            P("fs", "tp"),
            P("fs", "tp"),
            P("tp"),
            P("tp", "fs"),
            P(),
            P("fs", "tp"),
            P("fs", "tp"),
            P(None, "tp"),
            P(None, "tp"),
            P("tp", "fs"),
        ),
        out_specs=P(("grp", "fs"), "tp"),
        check_vma=False,
    )
```

```python
import functools

import jax
import jax.numpy as jnp
from jax import lax
from jax.experimental import pallas as pl
from jax.experimental.pallas import tpu as pltpu
from jax.sharding import PartitionSpec as P

HEAD = 128
EPS = 1e-06
MESH = pl.DeviceIdType.MESH
BF = jnp.bfloat16
F32 = jnp.float32
EARLY = 4
HALVED = 2


def qkvg_pieces(rows):
    return 4 if rows % 64 == 0 and rows > 64 else 1


def hidden_chunks(hidden):
    if hidden % 128:
        return [(0, hidden)]
    edges = list(range(0, hidden, 512)) + [hidden]
    return list(zip(edges[:-1], edges[1:]))


def kernel(cfg, x_hbm, mg, q_hbm, k_hbm, v_hbm, g_hbm, hg, ow_hbm, cg, up_hbm, sw_hbm, fu, fsw, dn_hbm,
           cos_ref, sin_ref, ld_ref, o_ref, *scratch):
    (wq, ob, ub, sb, db, xw, xn, xn1, qr, kr, vr, gr, ho, part, ra, st, rb, mw, mw1, lift, swit, hid,
     part1, ra1, st1, rb1, fin, loc, zs, zr, ys, yr, tks, tkr, fns, fnr) = scratch[:36]
    agx, agm, agn, rsm, rs0, rs1 = [scratch[36 + 4 * i:40 + 4 * i] for i in range(6)]
    n_g, n_f, n_t = cfg
    n_x = n_t // 2
    grp, z, t = lax.axis_index("grp"), lax.axis_index("fs"), lax.axis_index("tp")
    x, c = t // 2, t % 2
    partner = x * 2 + (1 - c)
    T, bw = x_hbm.shape
    D = bw * n_t
    RC = 256
    R = T // RC
    width = q_hbm.shape[1]
    heads = width // HEAD
    F = up_hbm.shape[1]
    fr = q_hbm.shape[0]
    slotw = ow_hbm.shape[1]
    per_block = bw // slotw
    n_j = slotw // 128
    w_j = per_block * 128
    chunks = hidden_chunks(F)

    is_end = jnp.logical_or(z == 0, z == n_f - 1)
    inner = jnp.logical_not(is_end)
    host = jnp.where(z == 0, 1, n_f - 2)
    guest = jnp.where(z == 1, 0, n_f - 1)
    second = None if n_f == 4 else jnp.logical_or(z == 1, z == n_f - 2)

    def when(cond):
        if cond is None:
            return lambda f: f()
        return pl.when(cond)

    def rows_of(r, size=RC):
        return pl.ds(r * size if isinstance(r, int) else pl.multiple_of(r * size, size), size)

    barrier = pltpu.get_barrier_semaphore()
    friends = [(grp, lax.rem(z + 1, n_f), t), (grp, lax.rem(z + n_f - 1, n_f), t), (grp, z, partner)]
    friends += [(lax.rem(grp + d, n_g), z, t) for d in range(1, n_g)]
    friends += [(grp, z, lax.rem(x + d, n_x) * 2 + c) for d in range(1, n_x)]
    for f in friends:
        pl.semaphore_signal(barrier, inc=1, device_id=f, device_id_type=MESH)

    zrow = pl.multiple_of(z * fr, fr)
    zcol = pl.multiple_of(z * 128, 128)
    local = [pltpu.make_async_copy(x_hbm, xw.at[t], loc.at[0])]
    for i, w in enumerate((q_hbm, k_hbm, v_hbm, g_hbm)):
        local.append(pltpu.make_async_copy(
            w, wq.at[pl.ds(zrow, fr), pl.ds(i * width, width)], loc.at[1 + i]))
    local.append(pltpu.make_async_copy(ow_hbm, ob.at[z], loc.at[5]))
    local.append(pltpu.make_async_copy(up_hbm, ub.at[pl.ds(zrow, fr), :], loc.at[6]))
    local.append(pltpu.make_async_copy(sw_hbm, sb.at[pl.ds(zrow, fr), :], loc.at[7]))
    for j in range(n_j):
        local.append(pltpu.make_async_copy(
            dn_hbm.at[:, pl.ds(j * 128, 128)], db.at[j, :, pl.ds(zcol, 128)], loc.at[8 + j]))
    for cp in local:
        cp.start()

    open_copies = [[]]

    def go(cp, cond=None):
        when(cond)(cp.start)
        open_copies[-1].append((cond, cp))

    def recv(cp, cond=None):
        when(cond)(cp.wait_recv)

    def drain():
        for cond, cp in open_copies[-1]:
            when(cond)(cp.wait_send)
        open_copies[-1].clear()

    pieces = []

    def add_rows(name, buf, slotted, shard, cols=None):
        half = shard // n_g
        count = qkvg_pieces(half) if name == "qkvg" else 1
        size = half // count
        for j in range(count):
            def ref(src, owner, j=j):
                if slotted:
                    return buf.at[src, pl.ds(pl.multiple_of(owner * half + j * size, size), size), :]
                rows = pl.ds(pl.multiple_of(src * shard + owner * half + j * size, size), size)
                return buf.at[rows, :] if cols is None else buf.at[rows, pl.ds(cols[0], cols[1] - cols[0])]
            pieces.append((name, ref))

    add_rows("qkvg", wq, False, fr)
    add_rows("out", ob, True, ow_hbm.shape[0])
    for k, cols in enumerate(chunks):
        for buf in (ub, sb):
            add_rows("ff%d" % k, buf, False, fr, cols if len(chunks) > 1 else None)
    for j in range(n_j):
        def down_ref(src, owner, j=j):
            half = F // n_g
            return db.at[j, pl.ds(pl.multiple_of(owner * half, half), half),
                         pl.ds(pl.multiple_of(src * 128, 128), 128)]
        pieces.append(("down%d" % j, down_ref))
    n_p = len(pieces)
    first_ff = min(i for i, pc in enumerate(pieces) if pc[0] == "ff0")

    def z_copy(p, src, step, way):
        ref = pieces[p][1](src, grp)
        return pltpu.make_async_remote_copy(
            src_ref=ref, dst_ref=ref, send_sem=zs.at[p, 2 * step + way], recv_sem=zr.at[p, src],
            device_id=(grp, z + (1 if way == 0 else -1), t), device_id_type=MESH)

    def y_copy(p, src, d):
        ref = pieces[p][1](src, grp)
        return pltpu.make_async_remote_copy(
            src_ref=ref, dst_ref=ref, send_sem=ys.at[p, src * n_g + d], recv_sem=yr.at[p, src * n_g + grp],
            device_id=(lax.rem(grp + d, n_g), z, t), device_id_type=MESH)

    def other_half(p, d):
        owner = lax.rem(grp + d, n_g)
        ref = pieces[p][1](z, owner)
        return pltpu.make_async_remote_copy(
            src_ref=ref, dst_ref=ref, send_sem=ys.at[p, z * n_g + d], recv_sem=yr.at[p, z * n_g + owner],
            device_id=(grp, host, t), device_id_type=MESH)

    def onward(p, way):
        edge = 1 if p >= first_ff else 0
        return z < n_f - 1 - edge if way == 0 else z > edge

    def own(p):
        for way in (0, 1):
            ahead = onward(p, way)
            go(z_copy(p, z, 0, way), jnp.logical_and(ahead, inner) if p >= first_ff else ahead)

    def whole(p):
        return not n_p - n_j <= p < n_p - n_j + min(HALVED, n_j - 1)

    def own_from_end(p):
        go(pltpu.make_async_remote_copy(
            src_ref=pieces[p][1](z, grp), dst_ref=pieces[p][1](z, grp), send_sem=ys.at[p, z * n_g],
            recv_sem=zr.at[p, z], device_id=(grp, host, t), device_id_type=MESH), is_end)
        if whole(p):
            for d in range(1, n_g):
                go(other_half(p, d), is_end)

    def event(p, s, kind):
        feed = p >= first_ff
        for way in (0, 1):
            src = z - s if way == 0 else z + s
            here = (src >= 0) if way == 0 else (src < n_f)
            if feed:
                here = jnp.logical_and(here, inner)
            far = True if s > 1 else z != (1 if way == 0 else n_f - 2)
            if kind == "near":
                here = jnp.logical_and(here, jnp.logical_not(far))
            if kind == "mid":
                here = jnp.logical_and(here, far)
            safe = jnp.clip(src, 0, n_f - 1)
            recv(z_copy(p, safe, s, way), here)
            go(z_copy(p, safe, s, way), jnp.logical_and(here, onward(p, way)))
            if kind != "near" or not whole(p):
                for d in range(1, n_g):
                    go(y_copy(p, safe, d), jnp.logical_and(here, far) if whole(p) else here)

    def arrive(p):
        for s in range(1, n_f):
            src = lax.rem(z + s, n_f)
            for d in range(1, n_g):
                owner = lax.rem(grp + d, n_g)
                ref = pieces[p][1](src, owner)
                pltpu.make_async_remote_copy(
                    src_ref=ref, dst_ref=ref, send_sem=ys.at[p, src * n_g],
                    recv_sem=yr.at[p, src * n_g + owner],
                    device_id=(owner, z, t), device_id_type=MESH).wait_recv()

    state = {"own": 0, "ev": 0}
    order = [(0, p, s, None) for s in range(1, n_f) for p in range(first_ff)]

    def when_due(p, s, kind):
        i, k = p - first_ff, p - (n_p - n_j)
        if kind == "mid":
            return 123 + 4 * k if k >= 0 else (71.2 + 5.6 * i if i < 3 else (93.6, 103.5, 113.3)[min(i, 5) - 3])
        near = (146.5, 150.5, 158.3, 166)[min(k, 3)] if k >= 0 else (75.2 + 11.2 * i if i < EARLY else 97 + 9.2 * i)
        if kind == "near":
            return near
        return near + (12.5 - 0.7 * i if i < EARLY else 4.5) + 6 * (s - 2)

    later = []
    for p in range(first_ff, n_p):
        later += [(when_due(p, 1, kind), p, 1, kind) for kind in ("mid", "near")]
        later += [(when_due(p, s, "far"), p, s, "far") for s in range(2, n_f - 1)]
    order += sorted(later)

    def send_own(upto):
        while state["own"] < min(upto, n_p):
            own(state["own"])
            state["own"] += 1

    def pump(count=1):
        for _ in range(count):
            if state["ev"] < len(order):
                _, p, s, kind = order[state["ev"]]
                event(p, s, kind)
                if (p, s) == (first_ff - 1, 1):
                    send_own(first_ff + 3)
                if kind == "near":
                    send_own(p + 4 if p - first_ff < 3 else n_p)
                state["ev"] += 1

    def pump_to(due):
        while state["ev"] < len(order) and order[state["ev"]][0] <= due:
            pump()

    def arrive_all(name):
        last = max(i for i, e in enumerate(order) if pieces[e[1]][0] == name)
        pump(max(0, last + 1 - state["ev"]))
        for i, pc in enumerate(pieces):
            if pc[0] == name:
                arrive(i)

    def ag_copy(buf, src_x, r, dest, ssem, rsem):
        ref = buf.at[src_x * 2 + c, rows_of(r), :]
        return pltpu.make_async_remote_copy(
            src_ref=ref, dst_ref=ref, send_sem=ssem, recv_sem=rsem,
            device_id=(grp, z, dest), device_id_type=MESH)

    def ag_start(buf, r, sems, cond=None):
        s1, r1, s2, r2 = sems
        for d in range(1, n_x):
            go(ag_copy(buf, x, r, lax.rem(x + d, n_x) * 2 + c, s1.at[d, r], r1.at[x, r]), cond)
        go(ag_copy(buf, x, r, partner, s2.at[x, r], r2.at[x, r]), cond)

    def ag_forward(buf, r, sems, cond=None):
        s1, r1, s2, r2 = sems
        for d in range(1, n_x):
            sx = lax.rem(x + d, n_x)
            recv(ag_copy(buf, sx, r, partner, s1.at[d, r], r1.at[sx, r]), cond)
            go(ag_copy(buf, sx, r, partner, s2.at[sx, r], r2.at[sx, r]), cond)

    def ag_finish(buf, r, sems, cond=None):
        s1, r1, s2, r2 = sems
        for sx in range(n_x):
            ref = buf.at[sx * 2 + (1 - c), rows_of(r), :]
            recv(pltpu.make_async_remote_copy(
                src_ref=ref, dst_ref=ref, send_sem=s2.at[sx, r], recv_sem=r2.at[sx, r],
                device_id=(grp, z, partner), device_id_type=MESH), cond)

    def norm_rows(src, gain, r, dst):
        def body(i, _):
            rows = rows_of(r * (RC // 64) + i, 64)
            total = jnp.zeros((64, 1), F32)
            for b in range(n_t):
                val = src[b, rows, :].astype(F32)
                total = total + jnp.sum(val * val, axis=-1, keepdims=True)
            inv = lax.rsqrt(total / D + EPS)
            for b in range(n_t):
                val = src[b, rows, :].astype(F32)
                dst[rows, b * bw:(b + 1) * bw] = (val * inv * gain[:, b * bw:(b + 1) * bw]).astype(BF)
            return 0
        lax.fori_loop(0, RC // 64, body, 0)

    def product(lhs, rhs, dst, block, r):
        for j in range(per_block):
            dst[block, rows_of(r), j * slotw:(j + 1) * slotw] = jnp.dot(
                lhs[rows_of(r), :], rhs[block * per_block + j], preferred_element_type=F32).astype(BF)

    def rs_copy(src_ref, dst_ref, dest, ssem, rsem):
        return pltpu.make_async_remote_copy(
            src_ref=src_ref, dst_ref=dst_ref, send_sem=ssem, recv_sem=rsem,
            device_id=(grp, z, dest), device_id_type=MESH)

    def mixer_reduce(emit):
        s1, r1, s2, r2 = rsm

        def to_partner(d, r):
            bx = lax.rem(x + d, n_x)
            return rs_copy(part.at[bx * 2 + 1 - c, rows_of(r), :], ra.at[d, rows_of(r), :],
                           partner, s1.at[d, r], r1.at[d, r])

        def across(d, r):
            return rs_copy(st.at[d - 1, rows_of(r), :], rb.at[d - 1, rows_of(r), :],
                           lax.rem(x + d, n_x) * 2 + c, s2.at[d, r], r2.at[d, r])

        sends = []

        def begin(cp):
            cp.start()
            sends.append(cp)

        def combine(d, r):
            bx = lax.rem(x + d, n_x)
            to_partner(d, r).wait_recv()
            st[d - 1, rows_of(r), :] = (part[bx * 2 + c, rows_of(r), :].astype(F32)
                                        + ra[d, rows_of(r), :].astype(F32)).astype(BF)
            begin(across(d, r))

        for r in range(R):
            project(r)
            for h in range(heads):
                retain(h, r)
            if r == 0:
                arrive_all("out")
            for d in range(1, n_x):
                bx = lax.rem(x + d, n_x)
                product(ho, ob, part, bx * 2 + 1 - c, r)
                begin(to_partner(d, r))
                product(ho, ob, part, bx * 2 + c, r)
            if r > 0:
                for d in range(1, n_x):
                    combine(d, r - 1)
            pump_to((0, 0, 75.3)[min(r, 2)])
        for r in range(R):
            product(ho, ob, part, x * 2 + 1 - c, r)
            begin(to_partner(0, r))
            if r == 0:
                for d in range(1, n_x):
                    combine(d, R - 1)
            product(ho, ob, part, x * 2 + c, r)
        for r in range(R):
            pump_to((77, 86.5, 89)[min(r, 2)])
            to_partner(0, r).wait_recv()
            total = part[t, rows_of(r), :].astype(F32) + ra[0, rows_of(r), :].astype(F32)
            for d in range(1, n_x):
                across(d, r).wait_recv()
                total = total + rb[d - 1, rows_of(r), :].astype(F32)
            emit(r, (xw[t, rows_of(r), :].astype(F32) + total).astype(BF))
        for cp in sends:
            cp.wait_send()

    pl.semaphore_wait(barrier, len(friends))
    local[0].wait()
    for r in range(R):
        ag_start(xw, r, agx)
    for cp in local[1:]:
        cp.wait()
    send_own(first_ff)
    for p in range(first_ff):
        for d in range(1, n_g):
            go(other_half(p, d), is_end)
    early = min(first_ff + EARLY, n_p - n_j)
    for p in range(first_ff, early):
        own_from_end(p)
    for r in range(R):
        pump(2 if r < 2 else 1)
        ag_forward(xw, r, agx)
    for r in range(R):
        ag_finish(xw, r, agx)
        norm_rows(xw, mg, r, xn)
        pump(1)
    arrive_all("qkvg")

    def project(r):
        rows = rows_of(r)
        lhs = xn[rows, :]
        for i, dst in enumerate((qr, kr, vr, gr)):
            val = jnp.dot(lhs, wq[:, i * width:(i + 1) * width], preferred_element_type=F32).astype(BF)
            if i >= 2:
                dst[rows, :] = val
                continue
            for h in range(heads):
                part_h = val[:, h * HEAD:(h + 1) * HEAD].astype(F32)
                dst[rows, h * HEAD:(h + 1) * HEAD] = (
                    part_h * cos_ref[rows, :] + pltpu.roll(part_h, HEAD // 2, 1) * sin_ref[rows, :]).astype(BF)

    def retain(h, r):
        cols = slice(h * HEAD, (h + 1) * HEAD)
        span = (r + 1) * RC
        qh = qr[r * RC:(r + 1) * RC, cols]
        scores = lax.dot_general(qh, kr[0:span, cols], (((1,), (1,)), ((), ())),
                                 preferred_element_type=F32)
        gap = (r * RC + lax.broadcasted_iota(jnp.int32, (RC, span), 0)
               - lax.broadcasted_iota(jnp.int32, (RC, span), 1))
        causal = gap >= 0
        rate = ld_ref[h:h + 1, 0:1]
        fade = jnp.where(causal, jnp.exp(rate * jnp.where(causal, gap, 0).astype(F32)), 0.0)
        weights = (scores * HEAD ** (-0.5) * fade).astype(BF)
        kept = jnp.dot(weights, vr[0:span, cols], preferred_element_type=F32)
        kept = kept * lax.rsqrt(jnp.mean(kept * kept, axis=-1, keepdims=True) + EPS)
        gate = gr[r * RC:(r + 1) * RC, cols].astype(F32)
        ho[r * RC:(r + 1) * RC, cols] = (kept * hg[:, cols] * (gate / (1.0 + jnp.exp(-gate)))).astype(BF)

    def token_copy(r, dest):
        return pltpu.make_async_remote_copy(
            src_ref=mw.at[t, rows_of(r), :], dst_ref=mw1.at[t, rows_of(r), :],
            send_sem=tks.at[r], recv_sem=tkr.at[r], device_id=(grp, dest, t), device_id_type=MESH)

    def emit_mixed(r, val):
        mw[t, rows_of(r), :] = val
        go(token_copy(r, host), is_end)
        ag_start(mw, r, agm, inner)

    mixer_reduce(emit_mixed)

    def fin_copy(j, dest):
        return pltpu.make_async_remote_copy(
            src_ref=fin.at[j], dst_ref=fin.at[j], send_sem=fns.at[j], recv_sem=fnr.at[j],
            device_id=(grp, dest, t), device_id_type=MESH)

    def cols_of(j):
        return slice(j * w_j, (j + 1) * w_j)

    def end_part():
        open_copies.append([])
        for p in range(early, n_p):
            own_from_end(p)
        for j in range(n_j):
            fin_copy(j, host).wait_recv()
            o_ref[:, cols_of(j)] = fin[j]
        drain()
        open_copies.pop()

    def widen(weights, lhs, dst, k):
        lo, hi = chunks[k]

        def body(r, _):
            dst[pl.ds(pl.multiple_of(16 + r * RC, 16), RC), 0:hi - lo] = jnp.dot(
                lhs[rows_of(r), :], weights[:, lo:hi], preferred_element_type=F32).astype(BF)
            return 0
        lax.fori_loop(0, R, body, 0)

    def conv(q, k):
        first, last = chunks[k]
        edges = list(range(0, last - first, 256)) + [last - first]

        def body(i, _):
            for lo, hi in zip(edges[:-1], edges[1:]):
                mixed = []
                for src, taps in ((lift, fu), (swit, fsw)):
                    val = src[pl.ds(pl.multiple_of(i * 64, 64), 80), lo:hi].astype(F32)
                    acc = pltpu.roll(val, 2, 0)[16:] * taps[0:1, first + lo:first + hi]
                    acc = acc + pltpu.roll(val, 1, 0)[16:] * taps[1:2, first + lo:first + hi]
                    mixed.append(acc + val[16:] * taps[2:3, first + lo:first + hi])
                a, b = mixed
                hid[q, rows_of(i, 64), first + lo:first + hi] = (a * (b / (1.0 + jnp.exp(-b)))).astype(BF)
            return 0
        lax.fori_loop(0, T // 64, body, 0)

    sides = ((part, ra, st, rb, rs0, None), (part1, ra1, st1, rb1, rs1, second))

    def to_partner(q, d, j):
        prt, r_a, _, _, sems, _ = sides[q]
        bx = lax.rem(x + d, n_x)
        return rs_copy(prt.at[bx * 2 + 1 - c, :, pl.ds(j * w_j, w_j)], r_a.at[d, :, pl.ds(j * w_j, w_j)],
                       partner, sems[0].at[d, j], sems[1].at[d, j])

    def across(q, d, j):
        _, _, stage, r_b, sems, _ = sides[q]
        return rs_copy(stage.at[d - 1, :, pl.ds(j * w_j, w_j)], r_b.at[d - 1, :, pl.ds(j * w_j, w_j)],
                       lax.rem(x + d, n_x) * 2 + c, sems[2].at[d, j], sems[3].at[d, j])

    def down(q, j):
        prt, cond = sides[q][0], sides[q][5]

        @when(cond)
        def _():
            def body(r, _):
                val = jnp.dot(hid[q, rows_of(r), :], db[j], preferred_element_type=F32).astype(BF)
                for src in range(n_f):
                    lo = (src % per_block) * slotw + j * 128
                    prt[src // per_block, rows_of(r), lo:lo + 128] = val[:, src * 128:(src + 1) * 128]
                return 0
            lax.fori_loop(0, R, body, 0)
        for d in list(range(1, n_x)) + [0]:
            go(to_partner(q, d, j), cond)

    def combine(q, j):
        prt, r_a, stage, _, _, cond = sides[q]
        for d in range(1, n_x):
            bx = lax.rem(x + d, n_x)
            recv(to_partner(q, d, j), cond)

            @when(cond)
            def _():
                stage[d - 1, :, cols_of(j)] = (prt[bx * 2 + c, :, cols_of(j)].astype(F32)
                                               + r_a[d, :, cols_of(j)].astype(F32)).astype(BF)
            go(across(q, d, j), cond)

    def finish(q, j):
        prt, r_a, _, r_b, _, cond = sides[q]
        base = (mw, mw1)[q]
        recv(to_partner(q, 0, j), cond)
        for d in range(1, n_x):
            recv(across(q, d, j), cond)

        @when(cond)
        def _():
            total = prt[t, :, cols_of(j)].astype(F32) + r_a[0, :, cols_of(j)].astype(F32)
            for d in range(1, n_x):
                total = total + r_b[d - 1, :, cols_of(j)].astype(F32)
            val = (base[t, :, cols_of(j)].astype(F32) + total).astype(BF)
            if q == 0:
                o_ref[:, cols_of(j)] = val
            else:
                fin[j] = val
        if q == 1:
            go(fin_copy(j, guest), cond)

    def inner_part():
        open_copies.append([])
        n_c = len(chunks)
        lift[0:16, :] = jnp.zeros((16, lift.shape[1]), BF)
        swit[0:16, :] = jnp.zeros((16, swit.shape[1]), BF)
        pump_to(98)
        for r in range(R):
            ag_forward(mw, r, agm)
            pump_to((103.6, 108.9, 111)[min(r, 2)])
        for r in range(R):
            ag_finish(mw, r, agm)
            norm_rows(mw, cg, r, xn)

        def feed(q, k, between=lambda: None):
            cond = sides[q][5]
            lhs = (xn, xn1)[q]
            when(cond)(lambda: widen(ub, lhs, lift, k))
            between()
            when(cond)(lambda: widen(sb, lhs, swit, k))
            when(cond)(lambda: conv(q, k))

        def token(r):
            recv(token_copy(r, guest), second)
            ag_start(mw1, r, agn, second)

        arrive_all("ff0")
        feed(0, 0, lambda: pump_to(113.5))
        token(0)
        pump_to(120)
        if R > 2:
            token(1)
        pump_to(124)
        for k in range(1, n_c - 1):
            arrive_all("ff%d" % k)
            if k == 1:
                token(R - 1)
            feed(0, k, lambda: pump_to(132))
        if n_c < 3:
            token(R - 1)
        for r in range(R):
            ag_forward(mw1, r, agn, second)
        pump_to(134)
        for r in range(R):
            ag_finish(mw1, r, agn, second)
            when(second)(lambda: norm_rows(mw1, cg, r, xn1))
        pump_to(135)
        for k in range(n_c - 1):
            feed(1, k, lambda: pump_to(139 if k == 0 else 143))
            pump_to(143 if k == 0 else 150.6)
        pump_to(151.5)
        if n_c > 1:
            arrive_all("ff%d" % (n_c - 1))
            feed(0, n_c - 1, lambda: pump_to(156))
            pump_to(159)
        arrive_all("down0")
        down(0, 0)
        pump_to(160)

        def between():
            combine(0, 0)
            pump_to(164)

        feed(1, n_c - 1, between)
        pump_to(167)
        down(1, 0)
        for j in range(1, n_j):
            combine(1, j - 1)
            arrive_all("down%d" % j)
            down(1, j)
            down(0, j)
            pump_to(1000)
            combine(0, j)
            finish(1, j - 1)
            finish(0, j - 1)
        combine(1, n_j - 1)
        finish(1, n_j - 1)
        finish(0, n_j - 1)
        drain()
        open_copies.pop()

    kept = dict(state)
    pl.when(is_end)(end_part)
    state.update(kept)
    pl.when(inner)(inner_part)
    drain()


def on_device(cfg, inputs, mixer_gain, query_weight, key_weight, value_weight, gate_weight, head_gain,
              out_weight, channel_gain, up_weight, switch_weight, filter_up, filter_switch, down_weight):
    n_g, n_f, n_t = cfg
    n_x = n_t // 2
    T, bw = inputs.shape
    D = bw * n_t
    fr, width = query_weight.shape
    heads = width // HEAD
    F = up_weight.shape[1]
    slotw = out_weight.shape[1]
    half = HEAD // 2
    per_block = bw // slotw
    n_j = slotw // 128
    assert n_f >= 4 and slotw % 128 == 0 and bw % slotw == 0 and (n_j == 1 or per_block == 1)
    frequency = 10000.0 ** (-jnp.arange(half, dtype=F32) * 2.0 / HEAD)
    angles = jnp.arange(T, dtype=jnp.int32).astype(F32)[:, None] * frequency[None, :]
    cosine, sine = jnp.cos(angles), jnp.sin(angles)
    cos2 = jnp.concatenate([cosine, cosine], axis=1)
    sin2 = jnp.concatenate([-sine, sine], axis=1)
    ids = (lax.axis_index("tp") * heads + jnp.arange(heads, dtype=jnp.int32)).astype(F32)
    rate = jnp.broadcast_to(jnp.log1p(-jnp.exp2(-5.0 - ids))[:, None], (heads, 128))

    chunks = hidden_chunks(F)
    span = max(hi - lo for lo, hi in chunks)
    n_p = qkvg_pieces(fr // n_g) + 1 + 2 * len(chunks) + n_j
    R = T // 256
    dma = pltpu.SemaphoreType.DMA
    anyspec = pl.BlockSpec(memory_space=pl.ANY)
    vspec = pl.BlockSpec(memory_space=pltpu.VMEM)
    act = pltpu.VMEM((n_t, T, bw), BF)
    flat = pltpu.VMEM((T, D), BF)
    xblk = pltpu.VMEM((n_x, T, bw), BF)
    yblk = pltpu.VMEM((n_x - 1, T, bw), BF)
    scratch = [
        pltpu.VMEM((D, 4 * width), BF),
        pltpu.VMEM((n_f,) + out_weight.shape, BF),
        pltpu.VMEM((D, F), BF),
        pltpu.VMEM((D, F), BF),
        pltpu.VMEM((n_j, F, n_f * 128), BF),
        act, flat, flat,
        pltpu.VMEM((T, width), BF), pltpu.VMEM((T, width), BF),
        pltpu.VMEM((T, width), BF), pltpu.VMEM((T, width), BF),
        pltpu.VMEM((T, width), BF),
        act, xblk, yblk, yblk,
        act, act,
        pltpu.VMEM((T + 16, span), BF), pltpu.VMEM((T + 16, span), BF), pltpu.VMEM((2, T, F), BF),
        act, xblk, yblk, yblk,
        pltpu.VMEM((n_j, T, per_block * 128), BF),
        dma((8 + n_j,)),
        dma((n_p, 2 * n_f)), dma((n_p, n_f)), dma((n_p, n_f * n_g)), dma((n_p, n_f * n_g)),
        dma((R,)), dma((R,)), dma((n_j,)), dma((n_j,)),
    ] + [dma((n_x, R))] * 16 + [dma((n_x, n_j))] * 8
    flops = 2 * T * (D * 4 * width + width * D + 3 * D * F)
    call = pl.pallas_call(
        functools.partial(kernel, cfg),
        out_shape=jax.ShapeDtypeStruct((T, bw), BF),
        in_specs=[anyspec, vspec, anyspec, anyspec, anyspec, anyspec, vspec, anyspec, vspec, anyspec, anyspec,
                  vspec, vspec, anyspec, vspec, vspec, vspec],
        out_specs=vspec,
        scratch_shapes=scratch,
        compiler_params=pltpu.CompilerParams(
            collective_id=0, has_side_effects=True, vmem_limit_bytes=67043328),
        cost_estimate=pl.CostEstimate(flops=flops, bytes_accessed=2 * (D * F * 3), transcendentals=0),
    )
    return call(inputs, mixer_gain[None, :], query_weight, key_weight, value_weight, gate_weight,
                head_gain[None, :], out_weight, channel_gain[None, :], up_weight, switch_weight,
                filter_up, filter_switch, down_weight, cos2, sin2, rate)


def solution(mesh):
    cfg = (mesh.shape["grp"], mesh.shape["fs"], mesh.shape["tp"])
    return jax.shard_map(
        functools.partial(on_device, cfg),
        mesh=mesh,
        in_specs=(
            P(("grp", "fs"), "tp"),
            P(),
            P("fs", "tp"),
            P("fs", "tp"),
            P("fs", "tp"),
            P("fs", "tp"),
            P("tp"),
            P("tp", "fs"),
            P(),
            P("fs", "tp"),
            P("fs", "tp"),
            P(None, "tp"),
            P(None, "tp"),
            P("tp", "fs"),
        ),
        out_specs=P(("grp", "fs"), "tp"),
        check_vma=False,
    )
```

```python
import functools

import jax
import jax.numpy as jnp
import numpy as np
from jax import lax
from jax.experimental import pallas as pl
from jax.experimental.pallas import tpu as pltpu
from jax.sharding import PartitionSpec as P

HEAD = 128
EPS = 1e-06
MESH = pl.DeviceIdType.MESH
BF = jnp.bfloat16
F32 = jnp.float32
EARLY = 4


def qkvg_pieces(rows):
    return 4 if rows % 64 == 0 and rows > 64 else 1


def hidden_chunks(hidden):
    if hidden % 128:
        return [(0, hidden)]
    edges = list(range(0, hidden, 512)) + [hidden]
    return list(zip(edges[:-1], edges[1:]))


def kernel(cfg, x_hbm, mg, q_hbm, k_hbm, v_hbm, g_hbm, hg, ow_hbm, cg, up_hbm, sw_hbm, fu, fsw, dn_hbm,
           turn_hbm, ld_ref, o_ref, *scratch):
    (wq, ob, ub, sb, db, xw, xn, xn1, qr, kr, vr, gr, ho, part, ra, st, rb, mw, mw1, lift, swit, hid,
     part1, ra1, st1, rb1, fin, turn, loc, zs, zr, ys, yr, tks, tkr, fns, fnr) = scratch[:37]
    agx, agm, agn, rsm, rs0, rs1 = [scratch[37 + 4 * i:41 + 4 * i] for i in range(6)]
    n_g, n_f, n_t = cfg
    n_x = n_t // 2
    grp, z, t = lax.axis_index("grp"), lax.axis_index("fs"), lax.axis_index("tp")
    x, c = t // 2, t % 2
    partner = x * 2 + (1 - c)
    T, bw = x_hbm.shape
    D = bw * n_t
    RC = 256
    R = T // RC
    width = q_hbm.shape[1]
    heads = width // HEAD
    F = up_hbm.shape[1]
    fr = q_hbm.shape[0]
    slotw = ow_hbm.shape[1]
    per_block = bw // slotw
    n_j = slotw // 128
    w_j = per_block * 128
    chunks = hidden_chunks(F)

    is_end = jnp.logical_or(z == 0, z == n_f - 1)
    inner = jnp.logical_not(is_end)
    host = jnp.where(z == 0, 1, n_f - 2)
    guest = jnp.where(z == 1, 0, n_f - 1)
    second = None if n_f == 4 else jnp.logical_or(z == 1, z == n_f - 2)

    def when(cond):
        if cond is None:
            return lambda f: f()
        return pl.when(cond)

    def rows_of(r, size=RC):
        return pl.ds(r * size if isinstance(r, int) else pl.multiple_of(r * size, size), size)

    barrier = pltpu.get_barrier_semaphore()
    friends = [(grp, lax.rem(z + 1, n_f), t), (grp, lax.rem(z + n_f - 1, n_f), t), (grp, z, partner)]
    friends += [(lax.rem(grp + d, n_g), z, t) for d in range(1, n_g)]
    friends += [(grp, z, lax.rem(x + d, n_x) * 2 + c) for d in range(1, n_x)]
    for f in friends:
        pl.semaphore_signal(barrier, inc=1, device_id=f, device_id_type=MESH)

    zrow = pl.multiple_of(z * fr, fr)
    zcol = pl.multiple_of(z * 128, 128)
    local = [pltpu.make_async_copy(x_hbm, xw.at[t], loc.at[0])]
    for i, w in enumerate((q_hbm, k_hbm, v_hbm, g_hbm)):
        local.append(pltpu.make_async_copy(
            w, wq.at[pl.ds(zrow, fr), pl.ds(i * width, width)], loc.at[1 + i]))
    local.append(pltpu.make_async_copy(ow_hbm, ob.at[z], loc.at[5]))
    local.append(pltpu.make_async_copy(up_hbm, ub.at[pl.ds(zrow, fr), :], loc.at[6]))
    local.append(pltpu.make_async_copy(sw_hbm, sb.at[pl.ds(zrow, fr), :], loc.at[7]))
    for j in range(n_j):
        local.append(pltpu.make_async_copy(
            dn_hbm.at[:, pl.ds(j * 128, 128)], db.at[j, :, pl.ds(zcol, 128)], loc.at[8 + j]))
    local.append(pltpu.make_async_copy(turn_hbm, turn, loc.at[8 + n_j]))
    for cp in local:
        cp.start()

    open_copies = [[]]

    def go(cp, cond=None):
        when(cond)(cp.start)
        open_copies[-1].append((cond, cp))

    def recv(cp, cond=None):
        when(cond)(cp.wait_recv)

    def drain():
        for cond, cp in open_copies[-1]:
            when(cond)(cp.wait_send)
        open_copies[-1].clear()

    pieces = []

    def add_rows(name, buf, slotted, shard, cols=None):
        half = shard // n_g
        count = qkvg_pieces(half) if name == "qkvg" else 1
        size = half // count
        for j in range(count):
            def ref(src, owner, j=j):
                if slotted:
                    return buf.at[src, pl.ds(pl.multiple_of(owner * half + j * size, size), size), :]
                rows = pl.ds(pl.multiple_of(src * shard + owner * half + j * size, size), size)
                return buf.at[rows, :] if cols is None else buf.at[rows, pl.ds(cols[0], cols[1] - cols[0])]
            pieces.append((name, ref))

    add_rows("qkvg", wq, False, fr)
    add_rows("out", ob, True, ow_hbm.shape[0])
    for k, cols in enumerate(chunks):
        for buf in (ub, sb):
            add_rows("ff%d" % k, buf, False, fr, cols if len(chunks) > 1 else None)
    for j in range(n_j):
        def down_ref(src, owner, j=j):
            half = F // n_g
            return db.at[j, pl.ds(pl.multiple_of(owner * half, half), half),
                         pl.ds(pl.multiple_of(src * 128, 128), 128)]
        pieces.append(("down%d" % j, down_ref))
    n_p = len(pieces)
    first_ff = min(i for i, pc in enumerate(pieces) if pc[0] == "ff0")

    def z_copy(p, src, step, way):
        ref = pieces[p][1](src, grp)
        return pltpu.make_async_remote_copy(
            src_ref=ref, dst_ref=ref, send_sem=zs.at[p, 2 * step + way], recv_sem=zr.at[p, src],
            device_id=(grp, z + (1 if way == 0 else -1), t), device_id_type=MESH)

    def y_slot(src, d):
        return src * (n_g - 1) + d - 1

    def y_copy(p, src, d):
        ref = pieces[p][1](src, grp)
        return pltpu.make_async_remote_copy(
            src_ref=ref, dst_ref=ref, send_sem=ys.at[p, y_slot(src, d)], recv_sem=yr.at[p, y_slot(src, n_g - d)],
            device_id=(lax.rem(grp + d, n_g), z, t), device_id_type=MESH)

    def other_half(p, d):
        owner = lax.rem(grp + d, n_g)
        ref = pieces[p][1](z, owner)
        return pltpu.make_async_remote_copy(
            src_ref=ref, dst_ref=ref, send_sem=ys.at[p, y_slot(z, d)], recv_sem=yr.at[p, y_slot(z, d)],
            device_id=(grp, host, t), device_id_type=MESH)

    def onward(p, way):
        edge = 1 if p >= first_ff else 0
        return z < n_f - 1 - edge if way == 0 else z > edge

    def own(p):
        for way in (0, 1):
            ahead = onward(p, way)
            go(z_copy(p, z, 0, way), jnp.logical_and(ahead, inner) if p >= first_ff else ahead)

    def whole(p):
        return not first_ff + EARLY <= p < n_p - n_j

    def own_from_end(p):
        go(pltpu.make_async_remote_copy(
            src_ref=pieces[p][1](z, grp), dst_ref=pieces[p][1](z, grp), send_sem=zs.at[p, 0],
            recv_sem=zr.at[p, z], device_id=(grp, host, t), device_id_type=MESH), is_end)
        if whole(p):
            for d in range(1, n_g):
                go(other_half(p, d), is_end)

    def event(p, s, kind):
        feed = p >= first_ff
        for way in (0, 1):
            src = z - s if way == 0 else z + s
            here = (src >= 0) if way == 0 else (src < n_f)
            if feed:
                here = jnp.logical_and(here, inner)
            far = True if s > 1 else z != (1 if way == 0 else n_f - 2)
            if kind == "near":
                here = jnp.logical_and(here, jnp.logical_not(far))
            if kind == "mid":
                here = jnp.logical_and(here, far)
            safe = jnp.clip(src, 0, n_f - 1)
            recv(z_copy(p, safe, min(s, n_f - 2), way), here)
            if s < n_f - 1:
                go(z_copy(p, safe, s, way), jnp.logical_and(here, onward(p, way)))
            if kind != "near" or not whole(p):
                for d in range(1, n_g):
                    go(y_copy(p, safe, d), jnp.logical_and(here, far) if whole(p) else here)

    def arrive(p):
        for s in range(1, n_f):
            src = lax.rem(z + s, n_f)
            for d in range(1, n_g):
                owner = lax.rem(grp + d, n_g)
                ref = pieces[p][1](src, owner)
                pltpu.make_async_remote_copy(
                    src_ref=ref, dst_ref=ref, send_sem=ys.at[p, y_slot(src, d)],
                    recv_sem=yr.at[p, y_slot(src, d)],
                    device_id=(owner, z, t), device_id_type=MESH).wait_recv()

    state = {"own": 0, "ev": 0}
    order = [(0, p, s, None) for s in range(1, n_f) for p in range(first_ff)]

    def when_due(p, s, kind):
        i, k = p - first_ff, p - (n_p - n_j)
        if kind == "mid":
            if k >= 0:
                return (124, 148.3, 156.1, 163.9)[min(k, 3)]
            return 71.2 + 5.6 * i if i < 3 else (93.6, 109.2, 119.5)[min(i, 5) - 3]
        near = 142.2 + 7.8 * k if k >= 0 else 75.2 + 11.2 * i if i < EARLY else 130.2 + 4.2 * (i - EARLY)
        if kind == "near":
            return near
        return near + (12.5 - 0.7 * i if i < EARLY else 6.4 if k < 0 else 6) + 6 * (s - 2)

    later = []
    for p in range(first_ff, n_p):
        later += [(when_due(p, 1, kind), p, 1, kind) for kind in ("mid", "near")]
        later += [(when_due(p, s, "far"), p, s, "far") for s in range(2, n_f - 1)]
    order += sorted(later)

    def send_own(upto):
        while state["own"] < min(upto, n_p):
            own(state["own"])
            state["own"] += 1

    def pump(count=1):
        for _ in range(count):
            if state["ev"] < len(order):
                _, p, s, kind = order[state["ev"]]
                event(p, s, kind)
                if (p, s) == (first_ff - 1, 1):
                    send_own(first_ff + 3)
                if kind == "near":
                    send_own(p + 4 if p - first_ff < 3 else n_p)
                state["ev"] += 1

    def pump_to(due):
        while state["ev"] < len(order) and order[state["ev"]][0] <= due:
            pump()

    def arrive_all(name):
        last = max(i for i, e in enumerate(order) if pieces[e[1]][0] == name)
        pump(max(0, last + 1 - state["ev"]))
        for i, pc in enumerate(pieces):
            if pc[0] == name:
                arrive(i)

    def ag_copy(buf, src_x, r, dest, ssem, rsem):
        ref = buf.at[src_x * 2 + c, rows_of(r), :]
        return pltpu.make_async_remote_copy(
            src_ref=ref, dst_ref=ref, send_sem=ssem, recv_sem=rsem,
            device_id=(grp, z, dest), device_id_type=MESH)

    def ag_start(buf, r, sems, cond=None):
        s1, r1, s2, r2 = sems
        for d in range(1, n_x):
            go(ag_copy(buf, x, r, lax.rem(x + d, n_x) * 2 + c, s1.at[d - 1, r], r1.at[x, r]), cond)
        go(ag_copy(buf, x, r, partner, s2.at[x, r], r2.at[x, r]), cond)

    def ag_forward(buf, r, sems, cond=None):
        s1, r1, s2, r2 = sems
        for d in range(1, n_x):
            sx = lax.rem(x + d, n_x)
            recv(ag_copy(buf, sx, r, partner, s1.at[d - 1, r], r1.at[sx, r]), cond)
            go(ag_copy(buf, sx, r, partner, s2.at[sx, r], r2.at[sx, r]), cond)

    def ag_finish(buf, r, sems, cond=None):
        s1, r1, s2, r2 = sems
        for sx in range(n_x):
            ref = buf.at[sx * 2 + (1 - c), rows_of(r), :]
            recv(pltpu.make_async_remote_copy(
                src_ref=ref, dst_ref=ref, send_sem=s2.at[sx, r], recv_sem=r2.at[sx, r],
                device_id=(grp, z, partner), device_id_type=MESH), cond)

    def norm_rows(src, gain, r, dst):
        def body(i, _):
            rows = rows_of(r * (RC // 64) + i, 64)
            total = jnp.zeros((64, 1), F32)
            for b in range(n_t):
                val = src[b, rows, :].astype(F32)
                total = total + jnp.sum(val * val, axis=-1, keepdims=True)
            inv = lax.rsqrt(total / D + EPS)
            for b in range(n_t):
                val = src[b, rows, :].astype(F32)
                dst[rows, b * bw:(b + 1) * bw] = (val * inv * gain[:, b * bw:(b + 1) * bw]).astype(BF)
            return 0
        lax.fori_loop(0, RC // 64, body, 0)

    def product(lhs, rhs, dst, block, r):
        for j in range(per_block):
            dst[block, rows_of(r), j * slotw:(j + 1) * slotw] = jnp.dot(
                lhs[rows_of(r), :], rhs[block * per_block + j], preferred_element_type=F32).astype(BF)

    def rs_copy(src_ref, dst_ref, dest, ssem, rsem):
        return pltpu.make_async_remote_copy(
            src_ref=src_ref, dst_ref=dst_ref, send_sem=ssem, recv_sem=rsem,
            device_id=(grp, z, dest), device_id_type=MESH)

    def mixer_reduce(emit):
        s1, r1, s2, r2 = rsm

        def to_partner(d, r):
            bx = lax.rem(x + d, n_x)
            return rs_copy(part.at[bx * 2 + 1 - c, rows_of(r), :], ra.at[d, rows_of(r), :],
                           partner, s1.at[d, r], r1.at[d, r])

        def across(d, r):
            return rs_copy(st.at[d - 1, rows_of(r), :], rb.at[d - 1, rows_of(r), :],
                           lax.rem(x + d, n_x) * 2 + c, s2.at[d - 1, r], r2.at[d - 1, r])

        sends = []

        def begin(cp):
            cp.start()
            sends.append(cp)

        def combine(d, r):
            bx = lax.rem(x + d, n_x)
            to_partner(d, r).wait_recv()
            st[d - 1, rows_of(r), :] = (part[bx * 2 + c, rows_of(r), :].astype(F32)
                                        + ra[d, rows_of(r), :].astype(F32)).astype(BF)
            begin(across(d, r))

        for r in range(R):
            project(r)
            for h in range(heads):
                retain(h, r)
            if r == 0:
                arrive_all("out")
            for d in range(1, n_x):
                bx = lax.rem(x + d, n_x)
                product(ho, ob, part, bx * 2 + 1 - c, r)
                begin(to_partner(d, r))
                product(ho, ob, part, bx * 2 + c, r)
            if r > 0:
                for d in range(1, n_x):
                    combine(d, r - 1)
            pump_to((0, 0, 75.3)[min(r, 2)])
        for r in range(R):
            product(ho, ob, part, x * 2 + 1 - c, r)
            begin(to_partner(0, r))
            if r == 0:
                for d in range(1, n_x):
                    combine(d, R - 1)
            product(ho, ob, part, x * 2 + c, r)
        for r in range(R):
            pump_to((77, 86.5, 89)[min(r, 2)])
            to_partner(0, r).wait_recv()
            total = part[t, rows_of(r), :].astype(F32) + ra[0, rows_of(r), :].astype(F32)
            for d in range(1, n_x):
                across(d, r).wait_recv()
                total = total + rb[d - 1, rows_of(r), :].astype(F32)
            emit(r, (xw[t, rows_of(r), :].astype(F32) + total).astype(BF))
        for cp in sends:
            cp.wait_send()

    pl.semaphore_wait(barrier, len(friends))
    local[0].wait()
    for r in range(R):
        ag_start(xw, r, agx)
    for cp in local[1:]:
        cp.wait()
    send_own(first_ff)
    for p in range(first_ff):
        for d in range(1, n_g):
            go(other_half(p, d), is_end)
    early = min(first_ff + EARLY, n_p - n_j)
    for p in range(first_ff, early):
        own_from_end(p)
    for r in range(R):
        pump(2 if r < 2 else 1)
        ag_forward(xw, r, agx)
    for r in range(R):
        ag_finish(xw, r, agx)
        norm_rows(xw, mg, r, xn)
        pump(1)
    arrive_all("qkvg")

    def project(r):
        rows = rows_of(r)
        lhs = xn[rows, :]
        both = turn[rows, :]
        swapped = pltpu.roll(both, HEAD // 2, 1)
        first_half = lax.broadcasted_iota(jnp.int32, (RC, HEAD), 1) < HEAD // 2
        cosine = jnp.where(first_half, both, swapped)
        sine = jnp.where(first_half, -swapped, both)
        for i, dst in enumerate((qr, kr, vr, gr)):
            val = jnp.dot(lhs, wq[:, i * width:(i + 1) * width], preferred_element_type=F32).astype(BF)
            if i >= 2:
                dst[rows, :] = val
                continue
            for h in range(heads):
                part_h = val[:, h * HEAD:(h + 1) * HEAD].astype(F32)
                dst[rows, h * HEAD:(h + 1) * HEAD] = (
                    part_h * cosine + pltpu.roll(part_h, HEAD // 2, 1) * sine).astype(BF)

    def retain(h, r):
        cols = slice(h * HEAD, (h + 1) * HEAD)
        span = (r + 1) * RC
        qh = qr[r * RC:(r + 1) * RC, cols]
        scores = lax.dot_general(qh, kr[0:span, cols], (((1,), (1,)), ((), ())),
                                 preferred_element_type=F32)
        gap = (r * RC + lax.broadcasted_iota(jnp.int32, (RC, span), 0)
               - lax.broadcasted_iota(jnp.int32, (RC, span), 1))
        causal = gap >= 0
        rate = ld_ref[pl.ds(t * heads + h, 1), 0:1]
        fade = jnp.where(causal, jnp.exp(rate * jnp.where(causal, gap, 0).astype(F32)), 0.0)
        weights = (scores * HEAD ** (-0.5) * fade).astype(BF)
        kept = jnp.dot(weights, vr[0:span, cols], preferred_element_type=F32)
        kept = kept * lax.rsqrt(jnp.mean(kept * kept, axis=-1, keepdims=True) + EPS)
        gate = gr[r * RC:(r + 1) * RC, cols].astype(F32)
        ho[r * RC:(r + 1) * RC, cols] = (kept * hg[:, cols] * (gate / (1.0 + jnp.exp(-gate)))).astype(BF)

    def token_copy(r, dest):
        return pltpu.make_async_remote_copy(
            src_ref=mw.at[t, rows_of(r), :], dst_ref=mw1.at[t, rows_of(r), :],
            send_sem=tks.at[r], recv_sem=tkr.at[r], device_id=(grp, dest, t), device_id_type=MESH)

    def emit_mixed(r, val):
        mw[t, rows_of(r), :] = val
        go(token_copy(r, host), is_end)
        ag_start(mw, r, agm, inner)

    mixer_reduce(emit_mixed)

    def fin_copy(j, dest):
        return pltpu.make_async_remote_copy(
            src_ref=fin.at[j], dst_ref=fin.at[j], send_sem=fns.at[j], recv_sem=fnr.at[j],
            device_id=(grp, dest, t), device_id_type=MESH)

    def cols_of(j):
        return slice(j * w_j, (j + 1) * w_j)

    def end_part():
        open_copies.append([])
        for p in range(early, n_p):
            own_from_end(p)
        for j in range(n_j):
            fin_copy(j, host).wait_recv()
            o_ref[:, cols_of(j)] = fin[j]
        drain()
        open_copies.pop()

    def widen(weights, lhs, dst, k):
        lo, hi = chunks[k]

        def body(r, _):
            dst[pl.ds(pl.multiple_of(16 + r * RC, 16), RC), 0:hi - lo] = jnp.dot(
                lhs[rows_of(r), :], weights[:, lo:hi], preferred_element_type=F32).astype(BF)
            return 0
        lax.fori_loop(0, R, body, 0)

    def conv(q, k):
        first, last = chunks[k]
        edges = list(range(0, last - first, 256)) + [last - first]

        def body(i, _):
            for lo, hi in zip(edges[:-1], edges[1:]):
                mixed = []
                for src, taps in ((lift, fu), (swit, fsw)):
                    val = src[pl.ds(pl.multiple_of(i * 64, 64), 80), lo:hi].astype(F32)
                    acc = pltpu.roll(val, 2, 0)[16:] * taps[0:1, first + lo:first + hi]
                    acc = acc + pltpu.roll(val, 1, 0)[16:] * taps[1:2, first + lo:first + hi]
                    mixed.append(acc + val[16:] * taps[2:3, first + lo:first + hi])
                a, b = mixed
                hid[q, rows_of(i, 64), first + lo:first + hi] = (a * (b / (1.0 + jnp.exp(-b)))).astype(BF)
            return 0
        lax.fori_loop(0, T // 64, body, 0)

    sides = ((part, ra, st, rb, rs0, None), (part1, ra1, st1, rb1, rs1, second))

    def to_partner(q, d, j):
        prt, r_a, _, _, sems, _ = sides[q]
        bx = lax.rem(x + d, n_x)
        return rs_copy(prt.at[bx * 2 + 1 - c, :, pl.ds(j * w_j, w_j)], r_a.at[d, :, pl.ds(j * w_j, w_j)],
                       partner, sems[0].at[d, j], sems[1].at[d, j])

    def across(q, d, j):
        _, _, stage, r_b, sems, _ = sides[q]
        return rs_copy(stage.at[d - 1, :, pl.ds(j * w_j, w_j)], r_b.at[d - 1, :, pl.ds(j * w_j, w_j)],
                       lax.rem(x + d, n_x) * 2 + c, sems[2].at[d - 1, j], sems[3].at[d - 1, j])

    def down(q, j):
        prt, cond = sides[q][0], sides[q][5]

        @when(cond)
        def _():
            def body(r, _):
                val = jnp.dot(hid[q, rows_of(r), :], db[j], preferred_element_type=F32).astype(BF)
                for src in range(n_f):
                    lo = (src % per_block) * slotw + j * 128
                    prt[src // per_block, rows_of(r), lo:lo + 128] = val[:, src * 128:(src + 1) * 128]
                return 0
            lax.fori_loop(0, R, body, 0)
        for d in list(range(1, n_x)) + [0]:
            go(to_partner(q, d, j), cond)

    def combine(q, j):
        prt, r_a, stage, _, _, cond = sides[q]
        for d in range(1, n_x):
            bx = lax.rem(x + d, n_x)
            recv(to_partner(q, d, j), cond)

            @when(cond)
            def _():
                stage[d - 1, :, cols_of(j)] = (prt[bx * 2 + c, :, cols_of(j)].astype(F32)
                                               + r_a[d, :, cols_of(j)].astype(F32)).astype(BF)
            go(across(q, d, j), cond)

    def finish(q, j):
        prt, r_a, _, r_b, _, cond = sides[q]
        base = (mw, mw1)[q]
        recv(to_partner(q, 0, j), cond)
        for d in range(1, n_x):
            recv(across(q, d, j), cond)

        @when(cond)
        def _():
            total = prt[t, :, cols_of(j)].astype(F32) + r_a[0, :, cols_of(j)].astype(F32)
            for d in range(1, n_x):
                total = total + r_b[d - 1, :, cols_of(j)].astype(F32)
            val = (base[t, :, cols_of(j)].astype(F32) + total).astype(BF)
            if q == 0:
                o_ref[:, cols_of(j)] = val
            else:
                fin[j] = val
        if q == 1:
            go(fin_copy(j, guest), cond)

    def inner_part():
        open_copies.append([])
        n_c = len(chunks)
        lift[0:16, :] = jnp.zeros((16, lift.shape[1]), BF)
        swit[0:16, :] = jnp.zeros((16, swit.shape[1]), BF)
        pump_to(98)
        for r in range(R):
            ag_forward(mw, r, agm)
            pump_to((103.6, 108.9, 111)[min(r, 2)])
        for r in range(R):
            ag_finish(mw, r, agm)
            norm_rows(mw, cg, r, xn)

        def feed(q, k, between=lambda: None):
            cond = sides[q][5]
            lhs = (xn, xn1)[q]
            when(cond)(lambda: widen(ub, lhs, lift, k))
            between()
            when(cond)(lambda: widen(sb, lhs, swit, k))
            when(cond)(lambda: conv(q, k))

        def token(r):
            recv(token_copy(r, guest), second)
            ag_start(mw1, r, agn, second)

        arrive_all("ff0")
        feed(0, 0, lambda: pump_to(113.5))
        token(0)
        pump_to(120)
        if R > 2:
            token(1)
        pump_to(124)
        for k in range(1, n_c - 1):
            arrive_all("ff%d" % k)
            if k == 1:
                token(R - 1)
            feed(0, k, lambda: pump_to(131))
        if n_c < 3:
            token(R - 1)
        for r in range(R):
            ag_forward(mw1, r, agn, second)
        pump_to(134.5)
        for r in range(R):
            ag_finish(mw1, r, agn, second)
            when(second)(lambda: norm_rows(mw1, cg, r, xn1))
        pump_to(135)
        for k in range(n_c - 1):
            feed(1, k, lambda: pump_to(139 if k == 0 else 143))
            pump_to(143 if k == 0 else 150.3)
        if n_c > 1:
            arrive_all("ff%d" % (n_c - 1))
            feed(0, n_c - 1, lambda: pump_to(152))
            pump_to(156.2)
        arrive_all("down0")
        down(0, 0)
        pump_to(158)

        def between():
            combine(0, 0)
            pump_to(158)

        feed(1, n_c - 1, between)
        pump_to(164)
        down(1, 0)
        for j in range(1, n_j):
            combine(1, j - 1)
            pump_to(156.4 + 7.6 * j)
            arrive_all("down%d" % j)
            down(1, j)
            down(0, j)
            pump_to(158.2 + 7.6 * j)
            combine(0, j)
            finish(1, j - 1)
            finish(0, j - 1)
        combine(1, n_j - 1)
        finish(1, n_j - 1)
        finish(0, n_j - 1)
        drain()
        open_copies.pop()

    kept = dict(state)
    pl.when(is_end)(end_part)
    state.update(kept)
    pl.when(inner)(inner_part)
    drain()


def on_device(cfg, inputs, mixer_gain, query_weight, key_weight, value_weight, gate_weight, head_gain,
              out_weight, channel_gain, up_weight, switch_weight, filter_up, filter_switch, down_weight):
    n_g, n_f, n_t = cfg
    n_x = n_t // 2
    T, bw = inputs.shape
    D = bw * n_t
    fr, width = query_weight.shape
    heads = width // HEAD
    F = up_weight.shape[1]
    slotw = out_weight.shape[1]
    half = HEAD // 2
    per_block = bw // slotw
    n_j = slotw // 128
    assert n_f >= 4 and slotw % 128 == 0 and bw % slotw == 0 and (n_j == 1 or per_block == 1)
    frequency = np.float32(10000.0) ** (-np.arange(half, dtype=np.float32) * np.float32(2.0) / np.float32(HEAD))
    angles = np.arange(T, dtype=np.float32)[:, None] * frequency[None, :]
    table = np.concatenate([np.cos(angles), np.sin(angles)], axis=1)
    rates = np.log1p(-np.exp2(-5.0 - np.arange(n_t * heads, dtype=np.float32)))
    rates = np.broadcast_to(rates[:, None], (n_t * heads, 128)).astype(np.float32)

    chunks = hidden_chunks(F)
    span = max(hi - lo for lo, hi in chunks)
    n_p = qkvg_pieces(fr // n_g) + 1 + 2 * len(chunks) + n_j
    R = T // 256
    dma = pltpu.SemaphoreType.DMA
    anyspec = pl.BlockSpec(memory_space=pl.ANY)
    vspec = pl.BlockSpec(memory_space=pltpu.VMEM)
    act = pltpu.VMEM((n_t, T, bw), BF)
    flat = pltpu.VMEM((T, D), BF)
    xblk = pltpu.VMEM((n_x, T, bw), BF)
    yblk = pltpu.VMEM((n_x - 1, T, bw), BF)
    scratch = [
        pltpu.VMEM((D, 4 * width), BF),
        pltpu.VMEM((n_f,) + out_weight.shape, BF),
        pltpu.VMEM((D, F), BF),
        pltpu.VMEM((D, F), BF),
        pltpu.VMEM((n_j, F, n_f * 128), BF),
        act, flat, flat,
        pltpu.VMEM((T, width), BF), pltpu.VMEM((T, width), BF),
        pltpu.VMEM((T, width), BF), pltpu.VMEM((T, width), BF),
        pltpu.VMEM((T, width), BF),
        act, xblk, yblk, yblk,
        act, act,
        pltpu.VMEM((T + 16, span), BF), pltpu.VMEM((T + 16, span), BF), pltpu.VMEM((2, T, F), BF),
        act, xblk, yblk, yblk,
        pltpu.VMEM((n_j, T, per_block * 128), BF),
        pltpu.VMEM((T, HEAD), F32),
        dma((9 + n_j,)),
        dma((n_p, 2 * (n_f - 1))), dma((n_p, n_f)),
        dma((n_p, n_f * (n_g - 1))), dma((n_p, n_f * (n_g - 1))),
        dma((R,)), dma((R,)), dma((n_j,)), dma((n_j,)),
    ] + ([dma((n_x - 1, R))] + [dma((n_x, R))] * 3) * 3 + ([dma((n_x, R))] * 2 + [dma((n_x - 1, R))] * 2) + (
        [dma((n_x, n_j))] * 2 + [dma((n_x - 1, n_j))] * 2) * 2
    flops = 2 * T * (D * 4 * width + width * D + 3 * D * F)
    call = pl.pallas_call(
        functools.partial(kernel, cfg),
        out_shape=jax.ShapeDtypeStruct((T, bw), BF),
        in_specs=[anyspec, vspec, anyspec, anyspec, anyspec, anyspec, vspec, anyspec, vspec, anyspec, anyspec,
                  vspec, vspec, anyspec, anyspec, vspec],
        out_specs=vspec,
        scratch_shapes=scratch,
        compiler_params=pltpu.CompilerParams(
            collective_id=0, has_side_effects=True, vmem_limit_bytes=67043328),
        cost_estimate=pl.CostEstimate(flops=flops, bytes_accessed=2 * (D * F * 3), transcendentals=0),
    )
    return call(inputs, mixer_gain[None, :], query_weight, key_weight, value_weight, gate_weight,
                head_gain[None, :], out_weight, channel_gain[None, :], up_weight, switch_weight,
                filter_up, filter_switch, down_weight, jnp.asarray(table), jnp.asarray(rates))


def solution(mesh):
    cfg = (mesh.shape["grp"], mesh.shape["fs"], mesh.shape["tp"])
    return jax.shard_map(
        functools.partial(on_device, cfg),
        mesh=mesh,
        in_specs=(
            P(("grp", "fs"), "tp"),
            P(),
            P("fs", "tp"),
            P("fs", "tp"),
            P("fs", "tp"),
            P("fs", "tp"),
            P("tp"),
            P("tp", "fs"),
            P(),
            P("fs", "tp"),
            P("fs", "tp"),
            P(None, "tp"),
            P(None, "tp"),
            P("tp", "fs"),
        ),
        out_specs=P(("grp", "fs"), "tp"),
        check_vma=False,
    )
```

```python
import functools

import jax
import jax.numpy as jnp
import numpy as np
from jax import lax
from jax.experimental import pallas as pl
from jax.experimental.pallas import tpu as pltpu
from jax.sharding import PartitionSpec as P

HEAD = 128
EPS = 1e-06
MESH = pl.DeviceIdType.MESH
BF = jnp.bfloat16
F32 = jnp.float32
EARLY = 4


def qkvg_pieces(rows):
    return 4 if rows % 64 == 0 and rows > 64 else 1


def hidden_chunks(hidden):
    if hidden % 128:
        return [(0, hidden)]
    edges = list(range(0, hidden, 512)) + [hidden]
    return list(zip(edges[:-1], edges[1:]))


def kernel(cfg, x_hbm, mg, q_hbm, k_hbm, v_hbm, g_hbm, hg, ow_hbm, cg, up_hbm, sw_hbm, fu, fsw, dn_hbm,
           turn_hbm, ld_ref, o_ref, *scratch):
    (wq, ob, ub, sb, db, xw, xn, xn1, qr, kr, vr, gr, ho, part, ra, st, rb, mw, mw1, lift, swit, hid,
     part1, ra1, st1, rb1, fin, turn, loc, zs, zr, ys, yr, tks, tkr, fns, fnr) = scratch[:37]
    agx, agm, agn, rsm, rs0, rs1 = [scratch[37 + 4 * i:41 + 4 * i] for i in range(6)]
    n_g, n_f, n_t = cfg
    n_x = n_t // 2
    grp, z, t = lax.axis_index("grp"), lax.axis_index("fs"), lax.axis_index("tp")
    x, c = t // 2, t % 2
    partner = x * 2 + (1 - c)
    T, bw = x_hbm.shape
    D = bw * n_t
    RC = 256
    R = T // RC
    width = q_hbm.shape[1]
    heads = width // HEAD
    F = up_hbm.shape[1]
    fr = q_hbm.shape[0]
    slotw = ow_hbm.shape[1]
    per_block = bw // slotw
    n_j = slotw // 128
    w_j = per_block * 128
    chunks = hidden_chunks(F)

    is_end = jnp.logical_or(z == 0, z == n_f - 1)
    inner = jnp.logical_not(is_end)
    host = jnp.where(z == 0, 1, n_f - 2)
    guest = jnp.where(z == 1, 0, n_f - 1)
    second = None if n_f == 4 else jnp.logical_or(z == 1, z == n_f - 2)

    def when(cond):
        if cond is None:
            return lambda f: f()
        return pl.when(cond)

    def rows_of(r, size=RC):
        return pl.ds(r * size if isinstance(r, int) else pl.multiple_of(r * size, size), size)

    barrier = pltpu.get_barrier_semaphore()
    friends = [(grp, lax.rem(z + 1, n_f), t), (grp, lax.rem(z + n_f - 1, n_f), t), (grp, z, partner)]
    friends += [(lax.rem(grp + d, n_g), z, t) for d in range(1, n_g)]
    friends += [(grp, z, lax.rem(x + d, n_x) * 2 + c) for d in range(1, n_x)]
    for f in friends:
        pl.semaphore_signal(barrier, inc=1, device_id=f, device_id_type=MESH)

    zrow = pl.multiple_of(z * fr, fr)
    zcol = pl.multiple_of(z * 128, 128)
    local = [pltpu.make_async_copy(x_hbm, xw.at[t], loc.at[0])]
    for i, w in enumerate((q_hbm, k_hbm, v_hbm, g_hbm)):
        local.append(pltpu.make_async_copy(
            w, wq.at[pl.ds(zrow, fr), pl.ds(i * width, width)], loc.at[1 + i]))
    local.append(pltpu.make_async_copy(ow_hbm, ob.at[z], loc.at[5]))
    local.append(pltpu.make_async_copy(up_hbm, ub.at[pl.ds(zrow, fr), :], loc.at[6]))
    local.append(pltpu.make_async_copy(sw_hbm, sb.at[pl.ds(zrow, fr), :], loc.at[7]))
    for j in range(n_j):
        local.append(pltpu.make_async_copy(
            dn_hbm.at[:, pl.ds(j * 128, 128)], db.at[j, :, pl.ds(zcol, 128)], loc.at[8 + j]))
    local.append(pltpu.make_async_copy(turn_hbm, turn, loc.at[8 + n_j]))
    for cp in local:
        cp.start()

    open_copies = [[]]

    def go(cp, cond=None):
        when(cond)(cp.start)
        open_copies[-1].append((cond, cp))

    def recv(cp, cond=None):
        when(cond)(cp.wait_recv)

    def drain():
        for cond, cp in open_copies[-1]:
            when(cond)(cp.wait_send)
        open_copies[-1].clear()

    pieces = []

    def add_rows(name, buf, slotted, shard, cols=None):
        half = shard // n_g
        count = qkvg_pieces(half) if name == "qkvg" else 1
        size = half // count
        for j in range(count):
            def ref(src, owner, j=j):
                if slotted:
                    return buf.at[src, pl.ds(pl.multiple_of(owner * half + j * size, size), size), :]
                rows = pl.ds(pl.multiple_of(src * shard + owner * half + j * size, size), size)
                return buf.at[rows, :] if cols is None else buf.at[rows, pl.ds(cols[0], cols[1] - cols[0])]
            pieces.append((name, ref))

    add_rows("qkvg", wq, False, fr)
    add_rows("out", ob, True, ow_hbm.shape[0])
    for k, cols in enumerate(chunks):
        for buf in (ub, sb):
            add_rows("ff%d" % k, buf, False, fr, cols if len(chunks) > 1 else None)
    for j in range(n_j):
        def down_ref(src, owner, j=j):
            half = F // n_g
            return db.at[j, pl.ds(pl.multiple_of(owner * half, half), half),
                         pl.ds(pl.multiple_of(src * 128, 128), 128)]
        pieces.append(("down%d" % j, down_ref))
    n_p = len(pieces)
    out_p = [pc[0] for pc in pieces].index("out")
    first_ff = min(i for i, pc in enumerate(pieces) if pc[0] == "ff0")

    def z_copy(p, src, step, way):
        ref = pieces[p][1](src, grp)
        return pltpu.make_async_remote_copy(
            src_ref=ref, dst_ref=ref, send_sem=zs.at[p, 2 * step + way], recv_sem=zr.at[p, src],
            device_id=(grp, z + (1 if way == 0 else -1), t), device_id_type=MESH)

    def y_slot(src, d):
        return src * (n_g - 1) + d - 1

    def y_copy(p, src, d):
        ref = pieces[p][1](src, grp)
        return pltpu.make_async_remote_copy(
            src_ref=ref, dst_ref=ref, send_sem=ys.at[p, y_slot(src, d)], recv_sem=yr.at[p, y_slot(src, n_g - d)],
            device_id=(lax.rem(grp + d, n_g), z, t), device_id_type=MESH)

    def other_half(p, d):
        owner = lax.rem(grp + d, n_g)
        ref = pieces[p][1](z, owner)
        return pltpu.make_async_remote_copy(
            src_ref=ref, dst_ref=ref, send_sem=ys.at[p, y_slot(z, d)], recv_sem=yr.at[p, y_slot(z, d)],
            device_id=(grp, host, t), device_id_type=MESH)

    def onward(p, way):
        edge = 1 if p >= first_ff else 0
        return z < n_f - 1 - edge if way == 0 else z > edge

    def own(p):
        for way in (0, 1):
            ahead = onward(p, way)
            go(z_copy(p, z, 0, way), jnp.logical_and(ahead, inner) if p >= out_p else ahead)

    def whole(p):
        return not first_ff + EARLY <= p < n_p - n_j

    def straight(p):
        return n_f == 4 and n_p - n_j <= p < n_p - n_j + min(2, n_j - 1)

    def relay(p, src, way, d):
        ref = pieces[p][1](src, lax.rem(grp + d, n_g))
        return pltpu.make_async_remote_copy(
            src_ref=ref, dst_ref=ref, send_sem=ys.at[p, y_slot(src, d)], recv_sem=yr.at[p, y_slot(src, d)],
            device_id=(grp, z + (1 if way == 0 else -1), t), device_id_type=MESH)

    def own_from_end(p):
        go(pltpu.make_async_remote_copy(
            src_ref=pieces[p][1](z, grp), dst_ref=pieces[p][1](z, grp), send_sem=zs.at[p, 0],
            recv_sem=zr.at[p, z], device_id=(grp, host, t), device_id_type=MESH), is_end)
        if whole(p):
            for d in range(1, n_g):
                go(other_half(p, d), is_end)

    def event(p, s, kind):
        feed = p >= first_ff
        for way in (0, 1):
            src = z - s if way == 0 else z + s
            here = (src >= 0) if way == 0 else (src < n_f)
            if feed:
                here = jnp.logical_and(here, inner)
            far = True if s > 1 else z != (1 if way == 0 else n_f - 2)
            if kind in ("near", "rest"):
                here = jnp.logical_and(here, jnp.logical_not(far))
            if kind == "mid":
                here = jnp.logical_and(here, far)
            safe = jnp.clip(src, 0, n_f - 1)
            if kind == "rest":
                for d in range(1, n_g):
                    recv(relay(p, safe, way, d), here)
                    go(relay(p, safe, way, d), jnp.logical_and(here, onward(p, way)))
                continue
            recv(z_copy(p, safe, min(s, n_f - 2), way), here)
            if s < n_f - 1:
                go(z_copy(p, safe, s, way), jnp.logical_and(here, onward(p, way)))
            if not (kind == "near" and whole(p)) and not (kind == "far" and straight(p)):
                for d in range(1, n_g):
                    go(y_copy(p, safe, d), jnp.logical_and(here, far) if whole(p) else here)

    def arrive(p):
        for s in range(1, n_f):
            src = lax.rem(z + s, n_f)
            for d in range(1, n_g):
                ref = pieces[p][1](src, lax.rem(grp + d, n_g))
                recv(pltpu.make_async_remote_copy(
                    src_ref=ref, dst_ref=ref, send_sem=ys.at[p, y_slot(src, d)],
                    recv_sem=yr.at[p, y_slot(src, d)],
                    device_id=(lax.rem(grp + d, n_g), z, t), device_id_type=MESH),
                    src != guest if straight(p) else None)

    state = {"own": 0, "ev": 0}
    order = []
    for s in range(1, n_f):
        order += [(0, p, s, None) for p in range(out_p)]
        if s < 3:
            order.append((0, out_p, 1, ("near", "mid")[s - 1]))
    order += [(0, out_p, s, "far") for s in range(2, n_f)]

    def when_due(p, s, kind):
        i, k = p - first_ff, p - (n_p - n_j)
        if kind == "mid":
            if k >= 0:
                return (122.2, 141.5, 151, 155)[min(k, 3)]
            return 71.2 + 5.6 * i if i < 3 else (93.2, 108.4, 118.2)[min(i, 5) - 3]
        near = 142.2 + 7.8 * k if k >= 0 else 69.6 + 11.2 * i if i < EARLY else 130.2 + 4.2 * (i - EARLY)
        if kind == "rest":
            return near
        if k >= 0:
            near -= 3.9
        if kind == "near":
            return near
        if i < EARLY:
            return (87.7, 98.9, 104.5, 114)[min(i, 3)] + 6 * (s - 2)
        return near + (6.4 if k < 0 else 8) + 6 * (s - 2)

    later = []
    for p in range(first_ff, n_p):
        later += [(when_due(p, 1, kind), p, 1, kind) for kind in ("mid", "near", "rest")[:3 if straight(p) else 2]]
        later += [(when_due(p, s, "far"), p, s, "far") for s in range(2, n_f - 1)]
    order += sorted(later)

    def send_own(upto):
        while state["own"] < min(upto, n_p):
            own(state["own"])
            state["own"] += 1

    def pump(count=1):
        for _ in range(count):
            if state["ev"] < len(order):
                _, p, s, kind = order[state["ev"]]
                event(p, s, kind)
                if (p, s) == (out_p - 1, 1):
                    send_own(first_ff)
                if kind == "near":
                    i = p - first_ff
                    send_own(first_ff + (3 if i < 0 else 4 if i < 2 else 5 if i < 3 else n_p))
                state["ev"] += 1

    def pump_to(due):
        while state["ev"] < len(order) and order[state["ev"]][0] <= due:
            pump()

    def arrive_all(name):
        last = max(i for i, e in enumerate(order) if pieces[e[1]][0] == name)
        pump(max(0, last + 1 - state["ev"]))
        for i, pc in enumerate(pieces):
            if pc[0] == name:
                arrive(i)

    def ag_copy(buf, src_x, r, dest, ssem, rsem):
        ref = buf.at[src_x * 2 + c, rows_of(r), :]
        return pltpu.make_async_remote_copy(
            src_ref=ref, dst_ref=ref, send_sem=ssem, recv_sem=rsem,
            device_id=(grp, z, dest), device_id_type=MESH)

    def ag_start(buf, r, sems, cond=None):
        s1, r1, s2, r2 = sems
        for d in range(1, n_x):
            go(ag_copy(buf, x, r, lax.rem(x + d, n_x) * 2 + c, s1.at[d - 1, r], r1.at[x, r]), cond)
        go(ag_copy(buf, x, r, partner, s2.at[x, r], r2.at[x, r]), cond)

    def ag_forward(buf, r, sems, cond=None):
        s1, r1, s2, r2 = sems
        for d in range(1, n_x):
            sx = lax.rem(x + d, n_x)
            recv(ag_copy(buf, sx, r, partner, s1.at[d - 1, r], r1.at[sx, r]), cond)
            go(ag_copy(buf, sx, r, partner, s2.at[sx, r], r2.at[sx, r]), cond)

    def ag_finish(buf, r, sems, cond=None):
        s1, r1, s2, r2 = sems
        for sx in range(n_x):
            ref = buf.at[sx * 2 + (1 - c), rows_of(r), :]
            recv(pltpu.make_async_remote_copy(
                src_ref=ref, dst_ref=ref, send_sem=s2.at[sx, r], recv_sem=r2.at[sx, r],
                device_id=(grp, z, partner), device_id_type=MESH), cond)

    def norm_rows(src, gain, r, dst):
        def body(i, _):
            rows = rows_of(r * (RC // 64) + i, 64)
            total = jnp.zeros((64, 1), F32)
            for b in range(n_t):
                val = src[b, rows, :].astype(F32)
                total = total + jnp.sum(val * val, axis=-1, keepdims=True)
            inv = lax.rsqrt(total / D + EPS)
            for b in range(n_t):
                val = src[b, rows, :].astype(F32)
                dst[rows, b * bw:(b + 1) * bw] = (val * inv * gain[:, b * bw:(b + 1) * bw]).astype(BF)
            return 0
        lax.fori_loop(0, RC // 64, body, 0)

    def product(lhs, rhs, dst, block, r):
        for j in range(per_block):
            dst[block, rows_of(r), j * slotw:(j + 1) * slotw] = jnp.dot(
                lhs[rows_of(r), :], rhs[block * per_block + j], preferred_element_type=F32).astype(BF)

    def rs_copy(src_ref, dst_ref, dest, ssem, rsem):
        return pltpu.make_async_remote_copy(
            src_ref=src_ref, dst_ref=dst_ref, send_sem=ssem, recv_sem=rsem,
            device_id=(grp, z, dest), device_id_type=MESH)

    def mixer_reduce(emit):
        s1, r1, s2, r2 = rsm

        def to_partner(d, r):
            bx = lax.rem(x + d, n_x)
            return rs_copy(part.at[bx * 2 + 1 - c, rows_of(r), :], ra.at[d, rows_of(r), :],
                           partner, s1.at[d, r], r1.at[d, r])

        def across(d, r):
            return rs_copy(st.at[d - 1, rows_of(r), :], rb.at[d - 1, rows_of(r), :],
                           lax.rem(x + d, n_x) * 2 + c, s2.at[d - 1, r], r2.at[d - 1, r])

        sends = []

        def begin(cp):
            cp.start()
            sends.append(cp)

        def combine(d, r):
            bx = lax.rem(x + d, n_x)
            to_partner(d, r).wait_recv()
            st[d - 1, rows_of(r), :] = (part[bx * 2 + c, rows_of(r), :].astype(F32)
                                        + ra[d, rows_of(r), :].astype(F32)).astype(BF)
            begin(across(d, r))

        for r in range(R):
            project(r)
            for h in range(heads):
                retain(h, r)
            if r == 0:
                arrive_all("out")
            for d in range(1, n_x):
                bx = lax.rem(x + d, n_x)
                product(ho, ob, part, bx * 2 + 1 - c, r)
                begin(to_partner(d, r))
                product(ho, ob, part, bx * 2 + c, r)
            if r > 0:
                for d in range(1, n_x):
                    combine(d, r - 1)
            pump_to((71.3, 71.3, 75.3)[min(r, 2)])
        for r in range(R):
            product(ho, ob, part, x * 2 + 1 - c, r)
            begin(to_partner(0, r))
            if r == 0:
                for d in range(1, n_x):
                    combine(d, R - 1)
            product(ho, ob, part, x * 2 + c, r)
        for r in range(R):
            pump_to((77, 86.5, 89)[min(r, 2)])
            to_partner(0, r).wait_recv()
            total = part[t, rows_of(r), :].astype(F32) + ra[0, rows_of(r), :].astype(F32)
            for d in range(1, n_x):
                across(d, r).wait_recv()
                total = total + rb[d - 1, rows_of(r), :].astype(F32)
            emit(r, (xw[t, rows_of(r), :].astype(F32) + total).astype(BF))
        for cp in sends:
            cp.wait_send()

    pl.semaphore_wait(barrier, len(friends))
    local[0].wait()
    for r in range(R):
        ag_start(xw, r, agx)
    for cp in local[1:5]:
        cp.wait()
    send_own(out_p)
    local[5].wait()
    for way in (0, 1):
        go(z_copy(out_p, z, 0, way), jnp.logical_and(onward(out_p, way), is_end))
    for p in range(first_ff):
        for d in range(1, n_g):
            go(other_half(p, d), is_end)
    for cp in local[6:]:
        cp.wait()
    early = min(first_ff + EARLY, n_p - n_j)
    for p in range(first_ff, early):
        own_from_end(p)
    for r in range(R):
        pump(2 if r < 2 else 1)
        ag_forward(xw, r, agx)
    for r in range(R):
        ag_finish(xw, r, agx)
        norm_rows(xw, mg, r, xn)
        pump(1)
    arrive_all("qkvg")

    def project(r):
        rows = rows_of(r)
        lhs = xn[rows, :]
        both = turn[rows, :]
        swapped = pltpu.roll(both, HEAD // 2, 1)
        first_half = lax.broadcasted_iota(jnp.int32, (RC, HEAD), 1) < HEAD // 2
        cosine = jnp.where(first_half, both, swapped)
        sine = jnp.where(first_half, -swapped, both)
        for i, dst in enumerate((qr, kr, vr, gr)):
            val = jnp.dot(lhs, wq[:, i * width:(i + 1) * width], preferred_element_type=F32).astype(BF)
            if i >= 2:
                dst[rows, :] = val
                continue
            for h in range(heads):
                part_h = val[:, h * HEAD:(h + 1) * HEAD].astype(F32)
                dst[rows, h * HEAD:(h + 1) * HEAD] = (
                    part_h * cosine + pltpu.roll(part_h, HEAD // 2, 1) * sine).astype(BF)

    def retain(h, r):
        cols = slice(h * HEAD, (h + 1) * HEAD)
        span = (r + 1) * RC
        qh = qr[r * RC:(r + 1) * RC, cols]
        scores = lax.dot_general(qh, kr[0:span, cols], (((1,), (1,)), ((), ())),
                                 preferred_element_type=F32)
        gap = (r * RC + lax.broadcasted_iota(jnp.int32, (RC, span), 0)
               - lax.broadcasted_iota(jnp.int32, (RC, span), 1))
        causal = gap >= 0
        rate = ld_ref[pl.ds(t * heads + h, 1), 0:1]
        fade = jnp.where(causal, jnp.exp(rate * jnp.where(causal, gap, 0).astype(F32)), 0.0)
        weights = (scores * HEAD ** (-0.5) * fade).astype(BF)
        kept = jnp.dot(weights, vr[0:span, cols], preferred_element_type=F32)
        kept = kept * lax.rsqrt(jnp.mean(kept * kept, axis=-1, keepdims=True) + EPS)
        gate = gr[r * RC:(r + 1) * RC, cols].astype(F32)
        ho[r * RC:(r + 1) * RC, cols] = (kept * hg[:, cols] * (gate / (1.0 + jnp.exp(-gate)))).astype(BF)

    def token_copy(r, dest):
        return pltpu.make_async_remote_copy(
            src_ref=mw.at[t, rows_of(r), :], dst_ref=mw1.at[t, rows_of(r), :],
            send_sem=tks.at[r], recv_sem=tkr.at[r], device_id=(grp, dest, t), device_id_type=MESH)

    def emit_mixed(r, val):
        mw[t, rows_of(r), :] = val
        go(token_copy(r, host), is_end)
        ag_start(mw, r, agm, inner)

    mixer_reduce(emit_mixed)

    def fin_copy(j, dest):
        return pltpu.make_async_remote_copy(
            src_ref=fin.at[j], dst_ref=fin.at[j], send_sem=fns.at[j], recv_sem=fnr.at[j],
            device_id=(grp, dest, t), device_id_type=MESH)

    def cols_of(j):
        return slice(j * w_j, (j + 1) * w_j)

    def end_part():
        open_copies.append([])
        for p in range(early, n_p):
            own_from_end(p)
        for j in range(n_j):
            fin_copy(j, host).wait_recv()
            o_ref[:, cols_of(j)] = fin[j]
        drain()
        open_copies.pop()

    def widen(weights, lhs, dst, k):
        lo, hi = chunks[k]

        def body(r, _):
            dst[pl.ds(pl.multiple_of(16 + r * RC, 16), RC), 0:hi - lo] = jnp.dot(
                lhs[rows_of(r), :], weights[:, lo:hi], preferred_element_type=F32).astype(BF)
            return 0
        lax.fori_loop(0, R, body, 0)

    def conv(q, k):
        first, last = chunks[k]
        edges = list(range(0, last - first, 256)) + [last - first]

        def body(i, _):
            for lo, hi in zip(edges[:-1], edges[1:]):
                mixed = []
                for src, taps in ((lift, fu), (swit, fsw)):
                    val = src[pl.ds(pl.multiple_of(i * 64, 64), 80), lo:hi].astype(F32)
                    acc = pltpu.roll(val, 2, 0)[16:] * taps[0:1, first + lo:first + hi]
                    acc = acc + pltpu.roll(val, 1, 0)[16:] * taps[1:2, first + lo:first + hi]
                    mixed.append(acc + val[16:] * taps[2:3, first + lo:first + hi])
                a, b = mixed
                hid[q, rows_of(i, 64), first + lo:first + hi] = (a * (b / (1.0 + jnp.exp(-b)))).astype(BF)
            return 0
        lax.fori_loop(0, T // 64, body, 0)

    sides = ((part, ra, st, rb, rs0, None), (part1, ra1, st1, rb1, rs1, second))

    def to_partner(q, d, j):
        prt, r_a, _, _, sems, _ = sides[q]
        bx = lax.rem(x + d, n_x)
        return rs_copy(prt.at[bx * 2 + 1 - c, :, pl.ds(j * w_j, w_j)], r_a.at[d, :, pl.ds(j * w_j, w_j)],
                       partner, sems[0].at[d, j], sems[1].at[d, j])

    def across(q, d, j):
        _, _, stage, r_b, sems, _ = sides[q]
        return rs_copy(stage.at[d - 1, :, pl.ds(j * w_j, w_j)], r_b.at[d - 1, :, pl.ds(j * w_j, w_j)],
                       lax.rem(x + d, n_x) * 2 + c, sems[2].at[d - 1, j], sems[3].at[d - 1, j])

    def down(q, j):
        prt, cond = sides[q][0], sides[q][5]

        @when(cond)
        def _():
            def body(r, _):
                val = jnp.dot(hid[q, rows_of(r), :], db[j], preferred_element_type=F32).astype(BF)
                for src in range(n_f):
                    lo = (src % per_block) * slotw + j * 128
                    prt[src // per_block, rows_of(r), lo:lo + 128] = val[:, src * 128:(src + 1) * 128]
                return 0
            lax.fori_loop(0, R, body, 0)
        for d in list(range(1, n_x)) + [0]:
            go(to_partner(q, d, j), cond)

    def combine(q, j):
        prt, r_a, stage, _, _, cond = sides[q]
        for d in range(1, n_x):
            bx = lax.rem(x + d, n_x)
            recv(to_partner(q, d, j), cond)

            @when(cond)
            def _():
                stage[d - 1, :, cols_of(j)] = (prt[bx * 2 + c, :, cols_of(j)].astype(F32)
                                               + r_a[d, :, cols_of(j)].astype(F32)).astype(BF)
            go(across(q, d, j), cond)

    def finish(q, j):
        prt, r_a, _, r_b, _, cond = sides[q]
        base = (mw, mw1)[q]
        recv(to_partner(q, 0, j), cond)
        for d in range(1, n_x):
            recv(across(q, d, j), cond)

        @when(cond)
        def _():
            total = prt[t, :, cols_of(j)].astype(F32) + r_a[0, :, cols_of(j)].astype(F32)
            for d in range(1, n_x):
                total = total + r_b[d - 1, :, cols_of(j)].astype(F32)
            val = (base[t, :, cols_of(j)].astype(F32) + total).astype(BF)
            if q == 0:
                o_ref[:, cols_of(j)] = val
            else:
                fin[j] = val
        if q == 1:
            go(fin_copy(j, guest), cond)

    def inner_part():
        open_copies.append([])
        n_c = len(chunks)
        lift[0:16, :] = jnp.zeros((16, lift.shape[1]), BF)
        swit[0:16, :] = jnp.zeros((16, swit.shape[1]), BF)
        pump_to(98)
        for r in range(R):
            ag_forward(mw, r, agm)
            pump_to((103.6, 108.9, 111)[min(r, 2)])
        for r in range(R):
            ag_finish(mw, r, agm)
            norm_rows(mw, cg, r, xn)

        def feed(q, k, between=lambda: None, later=lambda: None):
            cond = sides[q][5]
            lhs = (xn, xn1)[q]
            when(cond)(lambda: widen(ub, lhs, lift, k))
            between()
            when(cond)(lambda: widen(sb, lhs, swit, k))
            later()
            when(cond)(lambda: conv(q, k))

        def token(r):
            recv(token_copy(r, guest), second)
            ag_start(mw1, r, agn, second)

        arrive_all("ff0")
        feed(0, 0, lambda: pump_to(113.5))
        token(0)
        pump_to(120)
        if R > 2:
            token(1)
        pump_to(124)
        for k in range(1, n_c - 1):
            arrive_all("ff%d" % k)
            if k == 1:
                token(R - 1)
            feed(0, k, lambda: pump_to(125))
        pump_to(131)
        if n_c < 3:
            token(R - 1)
        for r in range(R):
            if r == R - 1:
                pump_to(134.5)
            ag_forward(mw1, r, agn, second)
        for r in range(R):
            ag_finish(mw1, r, agn, second)
            when(second)(lambda: norm_rows(mw1, cg, r, xn1))
        pump_to(135)
        for k in range(n_c - 1):
            feed(1, k, lambda: pump_to(139 if k == 0 else 146.2), lambda: pump_to(141.6 if k == 0 else 147))
            pump_to(143 if k == 0 else 150.3)
        if n_c > 1:
            arrive_all("ff%d" % (n_c - 1))
            feed(0, n_c - 1, lambda: pump_to(152))
            pump_to(156.2)
        arrive_all("down0")
        down(0, 0)
        pump_to(158)
        if n_j > 1:
            arrive_all("down1")
            down(0, 1)
        combine(0, 0)

        def between():
            pump_to(161.8)
            if n_j > 1:
                combine(0, 1)

        feed(1, n_c - 1, between, lambda: pump_to(165.7))
        rest = [(1, j) for j in range(n_j)] + [(0, j) for j in range(2, n_j)]
        last, ended = [], []

        def end(*items):
            for item in items:
                if item not in ended and item[1] < n_j:
                    finish(*item)
                    ended.append(item)

        for q, j in rest:
            if q == 1 and j > 1:
                pump_to(1000 if j == n_j - 1 else 166)
                if j == n_j - 1:
                    end((0, 0), (1, 0))
                arrive_all("down%d" % j)
            down(q, j)
            for item in last:
                combine(*item)
            last = [(q, j)]
            if j == 2 and q == 0:
                end((1, 1))
        for item in last:
            combine(*item)
        end((0, 0), (1, 0), (0, 1), *rest)
        drain()
        open_copies.pop()

    kept = dict(state)
    pl.when(is_end)(end_part)
    state.update(kept)
    pl.when(inner)(inner_part)
    drain()


def on_device(cfg, inputs, mixer_gain, query_weight, key_weight, value_weight, gate_weight, head_gain,
              out_weight, channel_gain, up_weight, switch_weight, filter_up, filter_switch, down_weight):
    n_g, n_f, n_t = cfg
    n_x = n_t // 2
    T, bw = inputs.shape
    D = bw * n_t
    fr, width = query_weight.shape
    heads = width // HEAD
    F = up_weight.shape[1]
    slotw = out_weight.shape[1]
    half = HEAD // 2
    per_block = bw // slotw
    n_j = slotw // 128
    assert n_f >= 4 and slotw % 128 == 0 and bw % slotw == 0 and (n_j == 1 or per_block == 1)
    frequency = np.float32(10000.0) ** (-np.arange(half, dtype=np.float32) * np.float32(2.0) / np.float32(HEAD))
    angles = np.arange(T, dtype=np.float32)[:, None] * frequency[None, :]
    table = np.concatenate([np.cos(angles), np.sin(angles)], axis=1)
    rates = np.log1p(-np.exp2(-5.0 - np.arange(n_t * heads, dtype=np.float32)))
    rates = np.broadcast_to(rates[:, None], (n_t * heads, 128)).astype(np.float32)

    chunks = hidden_chunks(F)
    span = max(hi - lo for lo, hi in chunks)
    n_p = qkvg_pieces(fr // n_g) + 1 + 2 * len(chunks) + n_j
    R = T // 256
    dma = pltpu.SemaphoreType.DMA
    anyspec = pl.BlockSpec(memory_space=pl.ANY)
    vspec = pl.BlockSpec(memory_space=pltpu.VMEM)
    act = pltpu.VMEM((n_t, T, bw), BF)
    flat = pltpu.VMEM((T, D), BF)
    xblk = pltpu.VMEM((n_x, T, bw), BF)
    yblk = pltpu.VMEM((n_x - 1, T, bw), BF)
    scratch = [
        pltpu.VMEM((D, 4 * width), BF),
        pltpu.VMEM((n_f,) + out_weight.shape, BF),
        pltpu.VMEM((D, F), BF),
        pltpu.VMEM((D, F), BF),
        pltpu.VMEM((n_j, F, n_f * 128), BF),
        act, flat, flat,
        pltpu.VMEM((T, width), BF), pltpu.VMEM((T, width), BF),
        pltpu.VMEM((T, width), BF), pltpu.VMEM((T, width), BF),
        pltpu.VMEM((T, width), BF),
        act, xblk, yblk, yblk,
        act, act,
        pltpu.VMEM((T + 16, span), BF), pltpu.VMEM((T + 16, span), BF), pltpu.VMEM((2, T, F), BF),
        act, xblk, yblk, yblk,
        pltpu.VMEM((n_j, T, per_block * 128), BF),
        pltpu.VMEM((T, HEAD), F32),
        dma((9 + n_j,)),
        dma((n_p, 2 * (n_f - 1))), dma((n_p, n_f)),
        dma((n_p, n_f * (n_g - 1))), dma((n_p, n_f * (n_g - 1))),
        dma((R,)), dma((R,)), dma((n_j,)), dma((n_j,)),
    ] + ([dma((n_x - 1, R))] + [dma((n_x, R))] * 3) * 3 + ([dma((n_x, R))] * 2 + [dma((n_x - 1, R))] * 2) + (
        [dma((n_x, n_j))] * 2 + [dma((n_x - 1, n_j))] * 2) * 2
    flops = 2 * T * (D * 4 * width + width * D + 3 * D * F)
    call = pl.pallas_call(
        functools.partial(kernel, cfg),
        out_shape=jax.ShapeDtypeStruct((T, bw), BF),
        in_specs=[anyspec, vspec, anyspec, anyspec, anyspec, anyspec, vspec, anyspec, vspec, anyspec, anyspec,
                  vspec, vspec, anyspec, anyspec, vspec],
        out_specs=vspec,
        scratch_shapes=scratch,
        compiler_params=pltpu.CompilerParams(
            collective_id=0, has_side_effects=True, vmem_limit_bytes=67043328),
        cost_estimate=pl.CostEstimate(flops=flops, bytes_accessed=2 * (D * F * 3), transcendentals=0),
    )
    return call(inputs, mixer_gain[None, :], query_weight, key_weight, value_weight, gate_weight,
                head_gain[None, :], out_weight, channel_gain[None, :], up_weight, switch_weight,
                filter_up, filter_switch, down_weight, jnp.asarray(table), jnp.asarray(rates))


def solution(mesh):
    cfg = (mesh.shape["grp"], mesh.shape["fs"], mesh.shape["tp"])
    return jax.shard_map(
        functools.partial(on_device, cfg),
        mesh=mesh,
        in_specs=(
            P(("grp", "fs"), "tp"),
            P(),
            P("fs", "tp"),
            P("fs", "tp"),
            P("fs", "tp"),
            P("fs", "tp"),
            P("tp"),
            P("tp", "fs"),
            P(),
            P("fs", "tp"),
            P("fs", "tp"),
            P(None, "tp"),
            P(None, "tp"),
            P("tp", "fs"),
        ),
        out_specs=P(("grp", "fs"), "tp"),
        check_vma=False,
    )
```

```python
import functools

import jax
import jax.numpy as jnp
import numpy as np
from jax import lax
from jax.experimental import pallas as pl
from jax.experimental.pallas import tpu as pltpu
from jax.sharding import PartitionSpec as P

HEAD = 128
EPS = 1e-06
MESH = pl.DeviceIdType.MESH
BF = jnp.bfloat16
F32 = jnp.float32
EARLY = 4


def qkvg_pieces(rows):
    return 4 if rows % 64 == 0 and rows > 64 else 1


def hidden_chunks(hidden):
    if hidden % 128:
        return [(0, hidden)]
    edges = list(range(0, hidden, 512)) + [hidden]
    return list(zip(edges[:-1], edges[1:]))


def kernel(cfg, x_hbm, mg, q_hbm, k_hbm, v_hbm, g_hbm, hg, ow_hbm, cg, up_hbm, sw_hbm, fu, fsw, dn_hbm,
           turn_hbm, ld_ref, o_ref, *scratch):
    (wq, ob, ub, sb, db, xw, xn, xn1, qr, kr, vr, gr, ho, part, ra, st, rb, mw, mw1, lift, swit, hid,
     part1, ra1, st1, rb1, fin, turn, loc, zs, zr, ys, yr, tks, tkr, fns, fnr) = scratch[:37]
    agx, agm, agn, rsm, rs0, rs1 = [scratch[37 + 4 * i:41 + 4 * i] for i in range(6)]
    n_g, n_f, n_t = cfg
    n_x = n_t // 2
    grp, z, t = lax.axis_index("grp"), lax.axis_index("fs"), lax.axis_index("tp")
    x, c = t // 2, t % 2
    partner = x * 2 + (1 - c)
    T, bw = x_hbm.shape
    D = bw * n_t
    RC = 256
    R = T // RC
    width = q_hbm.shape[1]
    heads = width // HEAD
    F = up_hbm.shape[1]
    fr = q_hbm.shape[0]
    slotw = ow_hbm.shape[1]
    per_block = bw // slotw
    n_j = slotw // 128
    w_j = per_block * 128
    chunks = hidden_chunks(F)

    is_end = jnp.logical_or(z == 0, z == n_f - 1)
    inner = jnp.logical_not(is_end)
    host = jnp.where(z == 0, 1, n_f - 2)
    guest = jnp.where(z == 1, 0, n_f - 1)
    second = None if n_f == 4 else jnp.logical_or(z == 1, z == n_f - 2)

    def when(cond):
        if cond is None:
            return lambda f: f()
        return pl.when(cond)

    def rows_of(r, size=RC):
        return pl.ds(r * size if isinstance(r, int) else pl.multiple_of(r * size, size), size)

    barrier = pltpu.get_barrier_semaphore()
    friends = [(grp, lax.rem(z + 1, n_f), t), (grp, lax.rem(z + n_f - 1, n_f), t), (grp, z, partner)]
    friends += [(lax.rem(grp + d, n_g), z, t) for d in range(1, n_g)]
    friends += [(grp, z, lax.rem(x + d, n_x) * 2 + c) for d in range(1, n_x)]
    for f in friends:
        pl.semaphore_signal(barrier, inc=1, device_id=f, device_id_type=MESH)

    zrow = pl.multiple_of(z * fr, fr)
    zcol = pl.multiple_of(z * 128, 128)
    local = [pltpu.make_async_copy(x_hbm, xw.at[t], loc.at[0])]
    for i, w in enumerate((q_hbm, k_hbm, v_hbm, g_hbm)):
        local.append(pltpu.make_async_copy(
            w, wq.at[pl.ds(zrow, fr), pl.ds(i * width, width)], loc.at[1 + i]))
    local.append(pltpu.make_async_copy(ow_hbm, ob.at[z], loc.at[5]))
    local.append(pltpu.make_async_copy(up_hbm, ub.at[pl.ds(zrow, fr), :], loc.at[6]))
    local.append(pltpu.make_async_copy(sw_hbm, sb.at[pl.ds(zrow, fr), :], loc.at[7]))
    for j in range(n_j):
        local.append(pltpu.make_async_copy(
            dn_hbm.at[:, pl.ds(j * 128, 128)], db.at[j, :, pl.ds(zcol, 128)], loc.at[8 + j]))
    local.append(pltpu.make_async_copy(turn_hbm, turn, loc.at[8 + n_j]))
    for cp in local:
        cp.start()

    open_copies = [[]]

    def go(cp, cond=None):
        when(cond)(cp.start)
        open_copies[-1].append((cond, cp))

    def recv(cp, cond=None):
        when(cond)(cp.wait_recv)

    def drain():
        for cond, cp in open_copies[-1]:
            when(cond)(cp.wait_send)
        open_copies[-1].clear()

    pieces = []

    def add_rows(name, buf, slotted, shard, cols=None):
        half = shard // n_g
        count = qkvg_pieces(half) if name == "qkvg" else 1
        size = half // count
        for j in range(count):
            def ref(src, owner, j=j):
                if slotted:
                    return buf.at[src, pl.ds(pl.multiple_of(owner * half + j * size, size), size), :]
                rows = pl.ds(pl.multiple_of(src * shard + owner * half + j * size, size), size)
                return buf.at[rows, :] if cols is None else buf.at[rows, pl.ds(cols[0], cols[1] - cols[0])]
            pieces.append((name, ref))

    add_rows("qkvg", wq, False, fr)
    add_rows("out", ob, True, ow_hbm.shape[0])
    for k, cols in enumerate(chunks):
        for buf in (ub, sb):
            add_rows("ff%d" % k, buf, False, fr, cols if len(chunks) > 1 else None)
    for j in range(n_j):
        def down_ref(src, owner, j=j):
            half = F // n_g
            return db.at[j, pl.ds(pl.multiple_of(owner * half, half), half),
                         pl.ds(pl.multiple_of(src * 128, 128), 128)]
        pieces.append(("down%d" % j, down_ref))
    n_p = len(pieces)
    out_p = [pc[0] for pc in pieces].index("out")
    first_ff = min(i for i, pc in enumerate(pieces) if pc[0] == "ff0")

    def z_copy(p, src, step, way):
        ref = pieces[p][1](src, grp)
        return pltpu.make_async_remote_copy(
            src_ref=ref, dst_ref=ref, send_sem=zs.at[p, 2 * step + way], recv_sem=zr.at[p, src],
            device_id=(grp, z + (1 if way == 0 else -1), t), device_id_type=MESH)

    def y_slot(src, d):
        return src * (n_g - 1) + d - 1

    def y_copy(p, src, d):
        ref = pieces[p][1](src, grp)
        return pltpu.make_async_remote_copy(
            src_ref=ref, dst_ref=ref, send_sem=ys.at[p, y_slot(src, d)], recv_sem=yr.at[p, y_slot(src, n_g - d)],
            device_id=(lax.rem(grp + d, n_g), z, t), device_id_type=MESH)

    def other_half(p, d):
        owner = lax.rem(grp + d, n_g)
        ref = pieces[p][1](z, owner)
        return pltpu.make_async_remote_copy(
            src_ref=ref, dst_ref=ref, send_sem=ys.at[p, y_slot(z, d)], recv_sem=yr.at[p, y_slot(z, d)],
            device_id=(grp, host, t), device_id_type=MESH)

    def onward(p, way):
        edge = 1 if p >= first_ff else 0
        return z < n_f - 1 - edge if way == 0 else z > edge

    def own(p):
        for way in (0, 1):
            ahead = onward(p, way)
            go(z_copy(p, z, 0, way), jnp.logical_and(ahead, inner) if p >= out_p else ahead)

    def whole(p):
        return not first_ff + EARLY <= p < n_p - n_j

    def straight(p):
        return n_f == 4 and n_p - n_j <= p < n_p - n_j + min(2, n_j - 1)

    def relay(p, src, way, d):
        ref = pieces[p][1](src, lax.rem(grp + d, n_g))
        return pltpu.make_async_remote_copy(
            src_ref=ref, dst_ref=ref, send_sem=ys.at[p, y_slot(src, d)], recv_sem=yr.at[p, y_slot(src, d)],
            device_id=(grp, z + (1 if way == 0 else -1), t), device_id_type=MESH)

    def own_from_end(p):
        go(pltpu.make_async_remote_copy(
            src_ref=pieces[p][1](z, grp), dst_ref=pieces[p][1](z, grp), send_sem=zs.at[p, 0],
            recv_sem=zr.at[p, z], device_id=(grp, host, t), device_id_type=MESH), is_end)
        if whole(p):
            for d in range(1, n_g):
                go(other_half(p, d), is_end)

    def event(p, s, kind):
        feed = p >= first_ff
        for way in (0, 1):
            src = z - s if way == 0 else z + s
            here = (src >= 0) if way == 0 else (src < n_f)
            if feed:
                here = jnp.logical_and(here, inner)
            far = True if s > 1 else z != (1 if way == 0 else n_f - 2)
            if kind in ("near", "rest"):
                here = jnp.logical_and(here, jnp.logical_not(far))
            if kind == "mid":
                here = jnp.logical_and(here, far)
            safe = jnp.clip(src, 0, n_f - 1)
            if kind == "rest":
                for d in range(1, n_g):
                    recv(relay(p, safe, way, d), here)
                    go(relay(p, safe, way, d), jnp.logical_and(here, onward(p, way)))
                continue
            recv(z_copy(p, safe, min(s, n_f - 2), way), here)
            if s < n_f - 1:
                go(z_copy(p, safe, s, way), jnp.logical_and(here, onward(p, way)))
            if not (kind == "near" and whole(p)) and not (kind == "far" and straight(p)):
                for d in range(1, n_g):
                    go(y_copy(p, safe, d), jnp.logical_and(here, far) if whole(p) else here)

    def arrive(p):
        for s in range(1, n_f):
            src = lax.rem(z + s, n_f)
            for d in range(1, n_g):
                ref = pieces[p][1](src, lax.rem(grp + d, n_g))
                recv(pltpu.make_async_remote_copy(
                    src_ref=ref, dst_ref=ref, send_sem=ys.at[p, y_slot(src, d)],
                    recv_sem=yr.at[p, y_slot(src, d)],
                    device_id=(lax.rem(grp + d, n_g), z, t), device_id_type=MESH),
                    src != guest if straight(p) else None)

    state = {"own": 0, "ev": 0}
    order = []
    for s in range(1, n_f):
        order += [(0, p, s, None) for p in range(out_p)]
        if s < 3:
            order.append((0, out_p, 1, ("near", "mid")[s - 1]))
    order += [(0, out_p, s, "far") for s in range(2, n_f)]

    def when_due(p, s, kind):
        i, k = p - first_ff, p - (n_p - n_j)
        if kind == "mid":
            if k >= 0:
                return (122.2, 141.5, 151, 155)[min(k, 3)]
            return 71.2 + 5.6 * i if i < 3 else (93.2, 108.4, 118.2)[min(i, 5) - 3]
        near = 142.2 + 7.8 * k if k >= 0 else 69.6 + 11.2 * i if i < EARLY else 130.2 + 4.2 * (i - EARLY)
        if kind == "rest":
            return near
        if k >= 0:
            near -= 3.9
        if kind == "near":
            return near
        if i < EARLY:
            return (87.7, 98.9, 104.5, 113.4)[min(i, 3)] + 6 * (s - 2)
        return near + (8 if k >= 0 else 4.7 if i == EARLY else 6.4) + 6 * (s - 2)

    later = []
    for p in range(first_ff, n_p):
        later += [(when_due(p, 1, kind), p, 1, kind) for kind in ("mid", "near", "rest")[:3 if straight(p) else 2]]
        later += [(when_due(p, s, "far"), p, s, "far") for s in range(2, n_f - 1)]
    order += sorted(later)

    def send_own(upto):
        while state["own"] < min(upto, n_p):
            own(state["own"])
            state["own"] += 1

    def pump(count=1):
        for _ in range(count):
            if state["ev"] < len(order):
                _, p, s, kind = order[state["ev"]]
                event(p, s, kind)
                if (p, s) == (out_p - 1, 1):
                    send_own(first_ff)
                if kind == "near":
                    i = p - first_ff
                    send_own(first_ff + (3 if i < 0 else 4 if i < 2 else 5 if i < 3 else n_p))
                state["ev"] += 1

    def pump_to(due):
        while state["ev"] < len(order) and order[state["ev"]][0] <= due:
            pump()

    def arrive_all(name):
        last = max(i for i, e in enumerate(order) if pieces[e[1]][0] == name)
        pump(max(0, last + 1 - state["ev"]))
        for i, pc in enumerate(pieces):
            if pc[0] == name:
                arrive(i)

    def ag_copy(buf, src_x, r, dest, ssem, rsem):
        ref = buf.at[src_x * 2 + c, rows_of(r), :]
        return pltpu.make_async_remote_copy(
            src_ref=ref, dst_ref=ref, send_sem=ssem, recv_sem=rsem,
            device_id=(grp, z, dest), device_id_type=MESH)

    def ag_start(buf, r, sems, cond=None):
        s1, r1, s2, r2 = sems
        for d in range(1, n_x):
            go(ag_copy(buf, x, r, lax.rem(x + d, n_x) * 2 + c, s1.at[d - 1, r], r1.at[x, r]), cond)
        go(ag_copy(buf, x, r, partner, s2.at[x, r], r2.at[x, r]), cond)

    def ag_forward(buf, r, sems, cond=None):
        s1, r1, s2, r2 = sems
        for d in range(1, n_x):
            sx = lax.rem(x + d, n_x)
            recv(ag_copy(buf, sx, r, partner, s1.at[d - 1, r], r1.at[sx, r]), cond)
            go(ag_copy(buf, sx, r, partner, s2.at[sx, r], r2.at[sx, r]), cond)

    def ag_finish(buf, r, sems, cond=None):
        s1, r1, s2, r2 = sems
        for sx in range(n_x):
            ref = buf.at[sx * 2 + (1 - c), rows_of(r), :]
            recv(pltpu.make_async_remote_copy(
                src_ref=ref, dst_ref=ref, send_sem=s2.at[sx, r], recv_sem=r2.at[sx, r],
                device_id=(grp, z, partner), device_id_type=MESH), cond)

    def norm_rows(src, gain, r, dst):
        def body(i, _):
            rows = rows_of(r * (RC // 64) + i, 64)
            total = jnp.zeros((64, 1), F32)
            for b in range(n_t):
                val = src[b, rows, :].astype(F32)
                total = total + jnp.sum(val * val, axis=-1, keepdims=True)
            inv = lax.rsqrt(total / D + EPS)
            for b in range(n_t):
                val = src[b, rows, :].astype(F32)
                dst[rows, b * bw:(b + 1) * bw] = (val * inv * gain[:, b * bw:(b + 1) * bw]).astype(BF)
            return 0
        lax.fori_loop(0, RC // 64, body, 0)

    def product(lhs, rhs, dst, block, r):
        for j in range(per_block):
            dst[block, rows_of(r), j * slotw:(j + 1) * slotw] = jnp.dot(
                lhs[rows_of(r), :], rhs[block * per_block + j], preferred_element_type=F32).astype(BF)

    def rs_copy(src_ref, dst_ref, dest, ssem, rsem):
        return pltpu.make_async_remote_copy(
            src_ref=src_ref, dst_ref=dst_ref, send_sem=ssem, recv_sem=rsem,
            device_id=(grp, z, dest), device_id_type=MESH)

    def mixer_reduce(emit):
        s1, r1, s2, r2 = rsm

        def to_partner(d, r):
            bx = lax.rem(x + d, n_x)
            return rs_copy(part.at[bx * 2 + 1 - c, rows_of(r), :], ra.at[d, rows_of(r), :],
                           partner, s1.at[d, r], r1.at[d, r])

        def across(d, r):
            return rs_copy(st.at[d - 1, rows_of(r), :], rb.at[d - 1, rows_of(r), :],
                           lax.rem(x + d, n_x) * 2 + c, s2.at[d - 1, r], r2.at[d - 1, r])

        sends = []

        def begin(cp):
            cp.start()
            sends.append(cp)

        def combine(d, r):
            bx = lax.rem(x + d, n_x)
            to_partner(d, r).wait_recv()
            st[d - 1, rows_of(r), :] = (part[bx * 2 + c, rows_of(r), :].astype(F32)
                                        + ra[d, rows_of(r), :].astype(F32)).astype(BF)
            begin(across(d, r))

        for r in range(R):
            project(r)
            for h in range(heads):
                retain(h, r)
            if r == 0:
                arrive_all("out")
            for d in range(1, n_x):
                bx = lax.rem(x + d, n_x)
                product(ho, ob, part, bx * 2 + 1 - c, r)
                begin(to_partner(d, r))
                product(ho, ob, part, bx * 2 + c, r)
            if r > 0:
                for d in range(1, n_x):
                    combine(d, r - 1)
            pump_to((71.3, 71.3, 75.3)[min(r, 2)])
        for r in range(R):
            product(ho, ob, part, x * 2 + 1 - c, r)
            begin(to_partner(0, r))
            if r == 0:
                for d in range(1, n_x):
                    combine(d, R - 1)
            product(ho, ob, part, x * 2 + c, r)
        for r in range(R):
            pump_to((77, 86.5, 89)[min(r, 2)])
            to_partner(0, r).wait_recv()
            total = part[t, rows_of(r), :].astype(F32) + ra[0, rows_of(r), :].astype(F32)
            for d in range(1, n_x):
                across(d, r).wait_recv()
                total = total + rb[d - 1, rows_of(r), :].astype(F32)
            emit(r, (xw[t, rows_of(r), :].astype(F32) + total).astype(BF))
        for cp in sends:
            cp.wait_send()

    pl.semaphore_wait(barrier, len(friends))
    local[0].wait()
    for r in range(R):
        ag_start(xw, r, agx)
    for cp in local[1:5]:
        cp.wait()
    send_own(out_p)
    local[5].wait()
    for way in (0, 1):
        go(z_copy(out_p, z, 0, way), jnp.logical_and(onward(out_p, way), is_end))
    for p in range(first_ff):
        for d in range(1, n_g):
            go(other_half(p, d), is_end)
    for cp in local[6:]:
        cp.wait()
    early = min(first_ff + EARLY, n_p - n_j)
    for p in range(first_ff, early):
        own_from_end(p)
    for r in range(R):
        pump(2 if r < 2 else 1)
        ag_forward(xw, r, agx)
    for r in range(R):
        ag_finish(xw, r, agx)
        norm_rows(xw, mg, r, xn)
        pump(1)
    arrive_all("qkvg")

    def project(r):
        rows = rows_of(r)
        lhs = xn[rows, :]
        both = turn[rows, :]
        swapped = pltpu.roll(both, HEAD // 2, 1)
        first_half = lax.broadcasted_iota(jnp.int32, (RC, HEAD), 1) < HEAD // 2
        cosine = jnp.where(first_half, both, swapped)
        sine = jnp.where(first_half, -swapped, both)
        for i, dst in enumerate((qr, kr, vr, gr)):
            val = jnp.dot(lhs, wq[:, i * width:(i + 1) * width], preferred_element_type=F32).astype(BF)
            if i >= 2:
                dst[rows, :] = val
                continue
            for h in range(heads):
                part_h = val[:, h * HEAD:(h + 1) * HEAD].astype(F32)
                dst[rows, h * HEAD:(h + 1) * HEAD] = (
                    part_h * cosine + pltpu.roll(part_h, HEAD // 2, 1) * sine).astype(BF)

    def retain(h, r):
        cols = slice(h * HEAD, (h + 1) * HEAD)
        span = (r + 1) * RC
        qh = qr[r * RC:(r + 1) * RC, cols]
        scores = lax.dot_general(qh, kr[0:span, cols], (((1,), (1,)), ((), ())),
                                 preferred_element_type=F32)
        gap = (r * RC + lax.broadcasted_iota(jnp.int32, (RC, span), 0)
               - lax.broadcasted_iota(jnp.int32, (RC, span), 1))
        causal = gap >= 0
        rate = ld_ref[pl.ds(t * heads + h, 1), 0:1]
        fade = jnp.where(causal, jnp.exp(rate * jnp.where(causal, gap, 0).astype(F32)), 0.0)
        weights = (scores * HEAD ** (-0.5) * fade).astype(BF)
        kept = jnp.dot(weights, vr[0:span, cols], preferred_element_type=F32)
        kept = kept * lax.rsqrt(jnp.mean(kept * kept, axis=-1, keepdims=True) + EPS)
        gate = gr[r * RC:(r + 1) * RC, cols].astype(F32)
        ho[r * RC:(r + 1) * RC, cols] = (kept * hg[:, cols] * (gate / (1.0 + jnp.exp(-gate)))).astype(BF)

    def token_copy(r, dest):
        return pltpu.make_async_remote_copy(
            src_ref=mw.at[t, rows_of(r), :], dst_ref=mw1.at[t, rows_of(r), :],
            send_sem=tks.at[r], recv_sem=tkr.at[r], device_id=(grp, dest, t), device_id_type=MESH)

    def emit_mixed(r, val):
        mw[t, rows_of(r), :] = val
        go(token_copy(r, host), is_end)
        ag_start(mw, r, agm, inner)

    mixer_reduce(emit_mixed)

    def fin_copy(j, dest):
        return pltpu.make_async_remote_copy(
            src_ref=fin.at[j], dst_ref=fin.at[j], send_sem=fns.at[j], recv_sem=fnr.at[j],
            device_id=(grp, dest, t), device_id_type=MESH)

    def cols_of(j):
        return slice(j * w_j, (j + 1) * w_j)

    def end_part():
        open_copies.append([])
        for p in range(early, n_p):
            own_from_end(p)
        for j in range(n_j):
            fin_copy(j, host).wait_recv()
            o_ref[:, cols_of(j)] = fin[j]
        drain()
        open_copies.pop()

    def widen(weights, lhs, dst, k):
        lo, hi = chunks[k]

        def body(r, _):
            dst[pl.ds(pl.multiple_of(16 + r * RC, 16), RC), 0:hi - lo] = jnp.dot(
                lhs[rows_of(r), :], weights[:, lo:hi], preferred_element_type=F32).astype(BF)
            return 0
        lax.fori_loop(0, R, body, 0)

    def conv(q, k):
        first, last = chunks[k]
        edges = list(range(0, last - first, 256)) + [last - first]

        def body(i, _):
            for lo, hi in zip(edges[:-1], edges[1:]):
                mixed = []
                for src, taps in ((lift, fu), (swit, fsw)):
                    val = src[pl.ds(pl.multiple_of(i * 64, 64), 80), lo:hi].astype(F32)
                    acc = pltpu.roll(val, 2, 0)[16:] * taps[0:1, first + lo:first + hi]
                    acc = acc + pltpu.roll(val, 1, 0)[16:] * taps[1:2, first + lo:first + hi]
                    mixed.append(acc + val[16:] * taps[2:3, first + lo:first + hi])
                a, b = mixed
                hid[q, rows_of(i, 64), first + lo:first + hi] = (a * (b / (1.0 + jnp.exp(-b)))).astype(BF)
            return 0
        lax.fori_loop(0, T // 64, body, 0)

    sides = ((part, ra, st, rb, rs0, None), (part1, ra1, st1, rb1, rs1, second))

    def to_partner(q, d, j):
        prt, r_a, _, _, sems, _ = sides[q]
        bx = lax.rem(x + d, n_x)
        return rs_copy(prt.at[bx * 2 + 1 - c, :, pl.ds(j * w_j, w_j)], r_a.at[d, :, pl.ds(j * w_j, w_j)],
                       partner, sems[0].at[d, j], sems[1].at[d, j])

    def across(q, d, j):
        _, _, stage, r_b, sems, _ = sides[q]
        return rs_copy(stage.at[d - 1, :, pl.ds(j * w_j, w_j)], r_b.at[d - 1, :, pl.ds(j * w_j, w_j)],
                       lax.rem(x + d, n_x) * 2 + c, sems[2].at[d - 1, j], sems[3].at[d - 1, j])

    def down(q, j):
        prt, cond = sides[q][0], sides[q][5]

        @when(cond)
        def _():
            def body(r, _):
                val = jnp.dot(hid[q, rows_of(r), :], db[j], preferred_element_type=F32).astype(BF)
                for src in range(n_f):
                    lo = (src % per_block) * slotw + j * 128
                    prt[src // per_block, rows_of(r), lo:lo + 128] = val[:, src * 128:(src + 1) * 128]
                return 0
            lax.fori_loop(0, R, body, 0)
        for d in list(range(1, n_x)) + [0]:
            go(to_partner(q, d, j), cond)

    def combine(q, j):
        prt, r_a, stage, _, _, cond = sides[q]
        for d in range(1, n_x):
            bx = lax.rem(x + d, n_x)
            recv(to_partner(q, d, j), cond)

            @when(cond)
            def _():
                stage[d - 1, :, cols_of(j)] = (prt[bx * 2 + c, :, cols_of(j)].astype(F32)
                                               + r_a[d, :, cols_of(j)].astype(F32)).astype(BF)
            go(across(q, d, j), cond)

    def finish(q, j):
        prt, r_a, _, r_b, _, cond = sides[q]
        base = (mw, mw1)[q]
        recv(to_partner(q, 0, j), cond)
        for d in range(1, n_x):
            recv(across(q, d, j), cond)

        @when(cond)
        def _():
            total = prt[t, :, cols_of(j)].astype(F32) + r_a[0, :, cols_of(j)].astype(F32)
            for d in range(1, n_x):
                total = total + r_b[d - 1, :, cols_of(j)].astype(F32)
            val = (base[t, :, cols_of(j)].astype(F32) + total).astype(BF)
            if q == 0:
                o_ref[:, cols_of(j)] = val
            else:
                fin[j] = val
        if q == 1:
            go(fin_copy(j, guest), cond)

    def inner_part():
        open_copies.append([])
        n_c = len(chunks)
        lift[0:16, :] = jnp.zeros((16, lift.shape[1]), BF)
        swit[0:16, :] = jnp.zeros((16, swit.shape[1]), BF)
        pump_to(98)
        for r in range(R):
            ag_forward(mw, r, agm)
            pump_to((103.6, 108.9, 111)[min(r, 2)])
        for r in range(R):
            ag_finish(mw, r, agm)
            norm_rows(mw, cg, r, xn)

        def feed(q, k, between=lambda: None, later=lambda: None):
            cond = sides[q][5]
            lhs = (xn, xn1)[q]
            when(cond)(lambda: widen(ub, lhs, lift, k))
            between()
            when(cond)(lambda: widen(sb, lhs, swit, k))
            later()
            when(cond)(lambda: conv(q, k))

        def token(r):
            recv(token_copy(r, guest), second)
            ag_start(mw1, r, agn, second)

        arrive_all("ff0")
        feed(0, 0, lambda: pump_to(113.5))
        token(0)
        pump_to(120)
        if R > 2:
            token(1)
        pump_to(124)
        for k in range(1, n_c - 1):
            arrive_all("ff%d" % k)
            if k == 1:
                token(R - 1)
            feed(0, k, lambda: pump_to(125))
        pump_to(131)
        if n_c < 3:
            token(R - 1)
        for r in range(R):
            if r == R - 1:
                pump_to(134.5)
            ag_forward(mw1, r, agn, second)
        for r in range(R):
            ag_finish(mw1, r, agn, second)
            when(second)(lambda: norm_rows(mw1, cg, r, xn1))
        pump_to(135)
        for k in range(n_c - 1):
            feed(1, k, lambda: pump_to(139 if k == 0 else 146.2), lambda: pump_to(141.6 if k == 0 else 147))
            pump_to(143 if k == 0 else 150.3)
        if n_c > 1:
            arrive_all("ff%d" % (n_c - 1))
            feed(0, n_c - 1, lambda: pump_to(152))
            pump_to(156.2)
        arrive_all("down0")
        down(0, 0)
        pump_to(158)
        if n_j > 1:
            arrive_all("down1")
            down(0, 1)
        combine(0, 0)

        def between():
            pump_to(161.8)
            if n_j > 1:
                combine(0, 1)

        feed(1, n_c - 1, between, lambda: pump_to(165.7))
        rest = [(1, j) for j in range(n_j)] + [(0, j) for j in range(2, n_j)]
        last, ended = [], []

        def end(*items):
            for item in items:
                if item not in ended and item[1] < n_j:
                    finish(*item)
                    ended.append(item)

        for q, j in rest:
            if q == 1 and j > 1:
                if j == n_j - 1:
                    for item in last:
                        combine(*item)
                    last = []
                pump_to(1000 if j == n_j - 1 else 166)
                if j == n_j - 1:
                    end((0, 0), (1, 0))
                arrive_all("down%d" % j)
            down(q, j)
            for item in last:
                combine(*item)
            last = [(q, j)]
            if j == 2 and q == 0:
                end((1, 1))
        for item in last:
            combine(*item)
        end((0, 0), (1, 0), (0, 1), *rest)
        drain()
        open_copies.pop()

    kept = dict(state)
    pl.when(is_end)(end_part)
    state.update(kept)
    pl.when(inner)(inner_part)
    drain()


def on_device(cfg, inputs, mixer_gain, query_weight, key_weight, value_weight, gate_weight, head_gain,
              out_weight, channel_gain, up_weight, switch_weight, filter_up, filter_switch, down_weight):
    n_g, n_f, n_t = cfg
    n_x = n_t // 2
    T, bw = inputs.shape
    D = bw * n_t
    fr, width = query_weight.shape
    heads = width // HEAD
    F = up_weight.shape[1]
    slotw = out_weight.shape[1]
    half = HEAD // 2
    per_block = bw // slotw
    n_j = slotw // 128
    assert n_f >= 4 and slotw % 128 == 0 and bw % slotw == 0 and (n_j == 1 or per_block == 1)
    frequency = np.float32(10000.0) ** (-np.arange(half, dtype=np.float32) * np.float32(2.0) / np.float32(HEAD))
    angles = np.arange(T, dtype=np.float32)[:, None] * frequency[None, :]
    table = np.concatenate([np.cos(angles), np.sin(angles)], axis=1)
    rates = np.log1p(-np.exp2(-5.0 - np.arange(n_t * heads, dtype=np.float32)))
    rates = np.broadcast_to(rates[:, None], (n_t * heads, 128)).astype(np.float32)

    chunks = hidden_chunks(F)
    span = max(hi - lo for lo, hi in chunks)
    n_p = qkvg_pieces(fr // n_g) + 1 + 2 * len(chunks) + n_j
    R = T // 256
    dma = pltpu.SemaphoreType.DMA
    anyspec = pl.BlockSpec(memory_space=pl.ANY)
    vspec = pl.BlockSpec(memory_space=pltpu.VMEM)
    act = pltpu.VMEM((n_t, T, bw), BF)
    flat = pltpu.VMEM((T, D), BF)
    xblk = pltpu.VMEM((n_x, T, bw), BF)
    yblk = pltpu.VMEM((n_x - 1, T, bw), BF)
    scratch = [
        pltpu.VMEM((D, 4 * width), BF),
        pltpu.VMEM((n_f,) + out_weight.shape, BF),
        pltpu.VMEM((D, F), BF),
        pltpu.VMEM((D, F), BF),
        pltpu.VMEM((n_j, F, n_f * 128), BF),
        act, flat, flat,
        pltpu.VMEM((T, width), BF), pltpu.VMEM((T, width), BF),
        pltpu.VMEM((T, width), BF), pltpu.VMEM((T, width), BF),
        pltpu.VMEM((T, width), BF),
        act, xblk, yblk, yblk,
        act, act,
        pltpu.VMEM((T + 16, span), BF), pltpu.VMEM((T + 16, span), BF), pltpu.VMEM((2, T, F), BF),
        act, xblk, yblk, yblk,
        pltpu.VMEM((n_j, T, per_block * 128), BF),
        pltpu.VMEM((T, HEAD), F32),
        dma((9 + n_j,)),
        dma((n_p, 2 * (n_f - 1))), dma((n_p, n_f)),
        dma((n_p, n_f * (n_g - 1))), dma((n_p, n_f * (n_g - 1))),
        dma((R,)), dma((R,)), dma((n_j,)), dma((n_j,)),
    ] + ([dma((n_x - 1, R))] + [dma((n_x, R))] * 3) * 3 + ([dma((n_x, R))] * 2 + [dma((n_x - 1, R))] * 2) + (
        [dma((n_x, n_j))] * 2 + [dma((n_x - 1, n_j))] * 2) * 2
    flops = 2 * T * (D * 4 * width + width * D + 3 * D * F)
    call = pl.pallas_call(
        functools.partial(kernel, cfg),
        out_shape=jax.ShapeDtypeStruct((T, bw), BF),
        in_specs=[anyspec, vspec, anyspec, anyspec, anyspec, anyspec, vspec, anyspec, vspec, anyspec, anyspec,
                  vspec, vspec, anyspec, anyspec, vspec],
        out_specs=vspec,
        scratch_shapes=scratch,
        compiler_params=pltpu.CompilerParams(
            collective_id=0, has_side_effects=True, vmem_limit_bytes=67043328),
        cost_estimate=pl.CostEstimate(flops=flops, bytes_accessed=2 * (D * F * 3), transcendentals=0),
    )
    return call(inputs, mixer_gain[None, :], query_weight, key_weight, value_weight, gate_weight,
                head_gain[None, :], out_weight, channel_gain[None, :], up_weight, switch_weight,
                filter_up, filter_switch, down_weight, jnp.asarray(table), jnp.asarray(rates))


def solution(mesh):
    cfg = (mesh.shape["grp"], mesh.shape["fs"], mesh.shape["tp"])
    return jax.shard_map(
        functools.partial(on_device, cfg),
        mesh=mesh,
        in_specs=(
            P(("grp", "fs"), "tp"),
            P(),
            P("fs", "tp"),
            P("fs", "tp"),
            P("fs", "tp"),
            P("fs", "tp"),
            P("tp"),
            P("tp", "fs"),
            P(),
            P("fs", "tp"),
            P("fs", "tp"),
            P(None, "tp"),
            P(None, "tp"),
            P("tp", "fs"),
        ),
        out_specs=P(("grp", "fs"), "tp"),
        check_vma=False,
    )
```
